32 devices in a mesh: sp: 8 (over z, x), tp: 4 (over y, core).
Axes of the slice: x: 2, y: 2, z: 4, core: 2. Of those that a mesh axis runs over, the one named last changes fastest.
Arguments:
- tokens: bfloat16 [1024, 2048], P('sp', 'tp'), may hold values from -6 to 6
- conv_value_weight: bfloat16 [2048, 1024], P('sp', 'tp'), may hold values from -0.125 to 0.125
- conv_gate_weight: bfloat16 [2048, 1024], P('sp', 'tp'), may hold values from -0.125 to 0.125
- conv_kernel: bfloat16 [31, 1024], P(None, 'tp'), may hold values from -16 to 16
- conv_norm_gain: float32 [1024], P('tp'), may hold values from 0.1 to 1.9
- query_weight: bfloat16 [2048, 2048], P('sp', 'tp'), may hold values from -0.125 to 0.125
- key_weight: bfloat16 [2048, 2048], P('sp', 'tp'), may hold values from -0.125 to 0.125
- value_weight: bfloat16 [2048, 2048], P('sp', 'tp'), may hold values from -0.125 to 0.125
- input_gate_weight: bfloat16 [2048, 8], P(None, 'tp'), may hold values from -0.125 to 0.125
- forget_gate_weight: bfloat16 [2048, 8], P(None, 'tp'), may hold values from -0.125 to 0.125
- input_offset: float32 [1024, 8], P('sp', 'tp'), may hold values from -4 to 210
- forget_offset: float32 [1024, 8], P('sp', 'tp'), may hold values from 0 to 30
- memory_norm_gain: float32 [2048], P('tp'), may hold values from 0.1 to 1.9
- conv_out_weight: bfloat16 [1024, 2048], P('tp', 'sp'), may hold values from -0.3125 to 0.3125
- memory_out_weight: bfloat16 [2048, 2048], P('tp', 'sp'), may hold values from -0.125 to 0.125
Outputs:
- mixed: bfloat16 [1024, 2048], P('sp', 'tp')
The draws below stay inside these ranges and needn't reach their ends.
All inputs are finite; a program needn't handle non-finite values.
Results may differ from the reference program's by a relative error of at most 0.03.
Values may be sent and summed in bfloat16 or wider, within the bound.
A program may use at most 128 MiB of HBM per device.

```python
import jax
import jax.numpy as jnp
from jax import lax

D = 2048
CONV = 1024
MEMORY_HEADS = 8
HEAD_DIM = 256
KERNEL = 31
BLOCK = 64
TOK_DEV = 128
SEQUENCE_TOKENS = 1024
GROUPS = 4


def draw_conv_kernel(key, part):
    key_rows = jax.random.split(jax.random.fold_in(key, 101), 2)
    channel = jnp.arange(CONV, dtype=jnp.float32) / CONV
    entries = jnp.clip(jax.random.normal(key_rows[0], (KERNEL, CONV), jnp.float32), -4.0, 4.0)
    rise = jnp.power(10.0, channel)
    factor = jnp.exp(jax.random.uniform(key_rows[1], (CONV,), jnp.float32, -0.35, 0.35))
    return (entries * rise * factor / jnp.sqrt(jnp.float32(KERNEL))).astype(jnp.bfloat16)


def draw_input_offset(key, part):
    key_rows = jax.random.split(jax.random.fold_in(key, 202), 1)
    position_offset = jnp.clip(jax.random.normal(key_rows[0], (SEQUENCE_TOKENS, MEMORY_HEADS), jnp.float32), -4.0, 4.0)
    return position_offset.astype(jnp.float32)


def draw_forget_offset(key, part):
    key_rows = jax.random.split(jax.random.fold_in(key, 303), 6)
    slow_head = jax.random.uniform(key_rows[0], (MEMORY_HEADS,)) < 0.5
    slow_level = jnp.log(jnp.float32(SEQUENCE_TOKENS)) + 3.0
    fast_level = jax.random.uniform(key_rows[1], (MEMORY_HEADS,), jnp.float32, 3.4, 4.6)
    level = jnp.where(slow_head, slow_level, fast_level)
    devices = SEQUENCE_TOKENS // TOK_DEV
    device_shift = jax.random.uniform(key_rows[2], (devices, 1, MEMORY_HEADS), jnp.float32, -0.7, 0.7)
    rough = 0.3 * jnp.clip(jax.random.normal(key_rows[3], (devices, TOK_DEV, MEMORY_HEADS), jnp.float32), -4.0, 4.0)
    position_offset = (level + device_shift + rough).reshape(SEQUENCE_TOKENS, MEMORY_HEADS)
    group_rows = jax.random.randint(key_rows[4], (3,), 0, SEQUENCE_TOKENS)
    token_positions = jnp.arange(SEQUENCE_TOKENS)
    token_group = jnp.any(token_positions[:, None] == group_rows[None, :], axis=1)
    group_level = jax.random.uniform(key_rows[5], (SEQUENCE_TOKENS, MEMORY_HEADS), jnp.float32, 0.9, 1.6)
    return jnp.where(token_group[:, None], group_level, position_offset).astype(jnp.float32)


def block_levels(key, dims, cuts, least, largest):
    level, own = 1.0, jax.random.fold_in(key, 6)
    for position, parts in cuts:
        draws = jnp.exp(jax.random.uniform(jax.random.fold_in(own, position), (parts,), jnp.float32, least / len(cuts), largest / len(cuts)))
        level = level * jnp.repeat(draws, dims[position] // parts).reshape([-1 if axis == position else 1 for axis in range(len(dims))])
    return level


def centred(stream_key, dims, width, limit, cuts=(), kind=jnp.bfloat16):
    drawn = width * jax.random.normal(stream_key, dims, jnp.float32)
    if cuts:
        drawn = drawn * block_levels(stream_key, dims, cuts, -0.22, 0.18)
    return jnp.clip(drawn, -limit, limit).astype(kind)


def setup_inputs(seed: int = 0) -> dict:
    keys = jax.random.split(jax.random.key(seed), 16)
    tokens = centred(keys[0], (SEQUENCE_TOKENS, D), 1.0, 6.0, ((0, 8), (1, 4)))
    conv_value_weight = centred(keys[1], (D, CONV), D ** -0.5, 0.125, ((0, 8), (1, 4)))
    conv_gate_weight = centred(keys[2], (D, CONV), D ** -0.5, 0.125, ((0, 8), (1, 4)))
    conv_kernel = draw_conv_kernel(jax.random.fold_in(keys[15], 71), 0)
    conv_norm_gain = jnp.clip(1.0 + 0.18 * jax.random.normal(keys[4], (CONV,), jnp.float32), 0.1, 1.9)
    query_weight = centred(keys[5], (D, MEMORY_HEADS * HEAD_DIM), D ** -0.5, 0.125, ((0, 8), (1, 4)))
    key_weight = centred(keys[6], (D, MEMORY_HEADS * HEAD_DIM), D ** -0.5, 0.125, ((0, 8), (1, 4)))
    value_weight = centred(keys[7], (D, MEMORY_HEADS * HEAD_DIM), D ** -0.5, 0.125, ((0, 8), (1, 4)))
    input_gate_weight = centred(keys[8], (D, MEMORY_HEADS), D ** -0.5, 0.125, ((1, 4),))
    forget_gate_weight = centred(keys[9], (D, MEMORY_HEADS), D ** -0.5, 0.125, ((1, 4),))
    input_offset = draw_input_offset(jax.random.fold_in(keys[15], 71), 0)
    forget_offset = draw_forget_offset(jax.random.fold_in(keys[15], 71), 0)
    memory_norm_gain = jnp.clip(1.0 + 0.18 * jax.random.normal(keys[12], (MEMORY_HEADS * HEAD_DIM,), jnp.float32), 0.1, 1.9)
    conv_out_weight = centred(keys[13], (CONV, D), (CONV // 3) ** -0.5, 0.3125, ((0, 4), (1, 8)))
    memory_out_weight = centred(keys[14], (MEMORY_HEADS * HEAD_DIM, D), (MEMORY_HEADS * HEAD_DIM) ** -0.5, 0.125, ((0, 4), (1, 8)))
    return {"tokens": tokens, "conv_value_weight": conv_value_weight, "conv_gate_weight": conv_gate_weight, "conv_kernel": conv_kernel, "conv_norm_gain": conv_norm_gain, "query_weight": query_weight, "key_weight": key_weight, "value_weight": value_weight, "input_gate_weight": input_gate_weight, "forget_gate_weight": forget_gate_weight, "input_offset": input_offset, "forget_offset": forget_offset, "memory_norm_gain": memory_norm_gain, "conv_out_weight": conv_out_weight, "memory_out_weight": memory_out_weight}


EPS = 1e-06

def block_step(carry, inputs):
    state, normal, level = carry
    query, key, value, gate_in, forget_log = inputs
    length = gate_in.shape[-1]
    scale = query.shape[-1] ** (-0.5)
    causal = jnp.tril(jnp.ones((length, length), dtype=bool))
    within = jnp.cumsum(forget_log, axis=-1)
    log_weight = within[:, :, None] - within[:, None, :] + gate_in[:, None, :]
    log_weight = jnp.where(causal, log_weight, -jnp.inf)
    carried = within + level[:, None]
    top = jnp.maximum(carried, lax.optimization_barrier(jnp.max(log_weight, axis=-1)))
    weight = jnp.exp(log_weight - top[:, :, None])
    carried_weight = jnp.exp(carried - top) * scale
    scores = jnp.einsum('htd,hsd->hts', query, key, preferred_element_type=jnp.float32) * (scale * weight)
    numer = jnp.einsum('hts,hse->hte', scores.astype(jnp.bfloat16), value, preferred_element_type=jnp.float32)
    numer = numer + carried_weight[:, :, None] * jnp.einsum('hed,htd->hte', state.astype(jnp.bfloat16), query, preferred_element_type=jnp.float32)
    denom = lax.optimization_barrier(jnp.sum(scores, axis=-1)) + carried_weight * jnp.einsum('hd,htd->ht', normal.astype(jnp.bfloat16), query, preferred_element_type=jnp.float32)
    result = numer / jnp.maximum(jnp.abs(denom), 1.0)[:, :, None]
    last = within[:, -1]
    end_log = last[:, None] - within + gate_in
    new_level = jnp.maximum(last + level, lax.optimization_barrier(jnp.max(end_log, axis=-1)))
    keep = jnp.exp(last + level - new_level)
    fresh = jnp.exp(end_log - new_level[:, None])
    scaled_key = (fresh[:, :, None] * key).astype(jnp.bfloat16)
    new_state = keep[:, None, None] * state + jnp.einsum('hse,hsd->hed', value, scaled_key, preferred_element_type=jnp.float32)
    new_normal = keep[:, None] * normal + lax.optimization_barrier(jnp.sum(scaled_key.astype(jnp.float32), axis=1))
    return ((new_state, new_normal, new_level), result)

def depthwise(extended, kernel):
    taps = kernel.shape[0]
    length = extended.shape[0] - taps + 1
    total = extended[0:length] * kernel[0]
    for index in range(1, taps):
        total = total + extended[index:index + length] * kernel[index]
    return total

def reference(tokens, conv_value_weight, conv_gate_weight, conv_kernel, conv_norm_gain, query_weight, key_weight, value_weight, input_gate_weight, forget_gate_weight, input_offset, forget_offset, memory_norm_gain, conv_out_weight, memory_out_weight):

    def project(weight):
        return jnp.dot(tokens, weight, preferred_element_type=jnp.float32)
    glu = (project(conv_value_weight) * jax.nn.sigmoid(project(conv_gate_weight))).astype(jnp.bfloat16)
    extended = jnp.concatenate([jnp.zeros((KERNEL - 1, CONV), jnp.float32), glu.astype(jnp.float32)], axis=0)
    conv = depthwise(extended, conv_kernel.astype(jnp.float32))
    mean = lax.optimization_barrier(jnp.mean(conv, axis=1, keepdims=True))
    variance = lax.optimization_barrier(jnp.mean(conv * conv, axis=1, keepdims=True)) - mean * mean
    conv_branch = jax.nn.silu((conv - mean) * lax.rsqrt(variance + EPS) * conv_norm_gain).astype(jnp.bfloat16)

    def to_heads(weight):
        return project(weight).astype(jnp.bfloat16).reshape(SEQUENCE_TOKENS, MEMORY_HEADS, HEAD_DIM).transpose(1, 0, 2)
    query = to_heads(query_weight)
    key = to_heads(key_weight)
    value = to_heads(value_weight)
    gate_in = (project(input_gate_weight) + input_offset).T
    forget_log = jax.nn.log_sigmoid(project(forget_gate_weight) + forget_offset).T
    blocks = SEQUENCE_TOKENS // BLOCK

    def split(array):
        return jnp.moveaxis(array.reshape((MEMORY_HEADS, blocks, BLOCK) + array.shape[2:]), 1, 0)
    start_state = (jnp.zeros((MEMORY_HEADS, HEAD_DIM, HEAD_DIM), jnp.float32), jnp.zeros((MEMORY_HEADS, HEAD_DIM), jnp.float32), jnp.full((MEMORY_HEADS,), -1e+30, jnp.float32))
    _, hidden = lax.scan(block_step, start_state, (split(query), split(key), split(value), split(gate_in), split(forget_log)))
    hidden = jnp.moveaxis(hidden, 0, 1).reshape(MEMORY_HEADS, SEQUENCE_TOKENS, HEAD_DIM)
    hidden = hidden * lax.rsqrt(lax.optimization_barrier(jnp.mean(hidden * hidden, axis=(0, 2), keepdims=True)) + EPS)
    hidden = hidden * memory_norm_gain.reshape(MEMORY_HEADS, 1, HEAD_DIM)
    memory_branch = hidden.transpose(1, 0, 2).reshape(SEQUENCE_TOKENS, MEMORY_HEADS * HEAD_DIM).astype(jnp.bfloat16)
    conv_share = CONV // GROUPS
    memory_share = MEMORY_HEADS * HEAD_DIM // GROUPS
    mixed = jnp.zeros((SEQUENCE_TOKENS, D), jnp.float32)
    for group in range(GROUPS):
        conv_rows = slice(group * conv_share, (group + 1) * conv_share)
        memory_rows = slice(group * memory_share, (group + 1) * memory_share)
        partial_value = jnp.dot(conv_branch[:, conv_rows], conv_out_weight[conv_rows], preferred_element_type=jnp.float32)
        partial_value = partial_value + jnp.dot(memory_branch[:, memory_rows], memory_out_weight[memory_rows], preferred_element_type=jnp.float32)
        rounded = lax.optimization_barrier(partial_value.astype(jnp.bfloat16))
        mixed = mixed + rounded.astype(jnp.float32)
    return mixed.astype(jnp.bfloat16)
```

```python
import jax
import jax.numpy as jnp
from jax import lax
from jax.sharding import PartitionSpec as P

BLOCK = 64


EPS = 1e-06
LOWEST_LEVEL = -1e30


def shifted_2(value, axis, steps):
    count = lax.axis_size(axis)
    leading, last = (max(0, -steps), min(count, count - steps))
    return lax.ppermute(value, axis, [(source, source + steps) for source in range(leading, last)])


def carried_in(shard, axis, join, neutral):
    place = lax.axis_index(axis)
    gathered = jax.tree.map(
        lambda a, kind: lax.all_gather(a.astype(kind), axis),
        shard,
        (jnp.bfloat16, jnp.bfloat16, jnp.bfloat16, jnp.bfloat16),
    )
    state = jax.tree.map(lambda a, e: jnp.zeros_like(a) + jnp.asarray(e, a.dtype), shard, neutral)

    def one(step, state):
        return join(
            state,
            jax.tree.map(
                lambda a, own: lax.dynamic_index_in_dim(a, step, 0, False).astype(own.dtype),
                gathered,
                shard,
            ),
        )

    return lax.fori_loop(0, place, one, state)


def block_step(carry, inputs):
    state, normal, level = carry
    query, key, value, gate_in, forget_log = inputs
    length = gate_in.shape[-1]
    scale = query.shape[-1] ** (-0.5)
    causal = jnp.tril(jnp.ones((length, length), dtype=bool))
    within = jnp.cumsum(forget_log, axis=-1)
    log_weight = within[:, :, None] - within[:, None, :] + gate_in[:, None, :]
    log_weight = jnp.where(causal, log_weight, -jnp.inf)
    carried = within + level[:, None]
    top = jnp.maximum(carried, jnp.max(log_weight, axis=-1))
    weight = jnp.exp(log_weight - top[:, :, None])
    carried_weight = jnp.exp(carried - top) * scale
    scores = jnp.einsum("htd,hsd->hts", query, key, preferred_element_type=jnp.float32) * (
        scale * weight
    )
    numer = jnp.einsum(
        "hts,hse->hte", scores.astype(jnp.bfloat16), value, preferred_element_type=jnp.float32
    )
    numer = numer + carried_weight[:, :, None] * jnp.einsum(
        "hed,htd->hte", state.astype(jnp.bfloat16), query, preferred_element_type=jnp.float32
    )
    denom = jnp.sum(scores, axis=-1) + carried_weight * jnp.einsum(
        "hd,htd->ht", normal.astype(jnp.bfloat16), query, preferred_element_type=jnp.float32
    )
    result = numer / jnp.maximum(jnp.abs(denom), 1.0)[:, :, None]
    last = within[:, -1]
    end_log = last[:, None] - within + gate_in
    new_level = jnp.maximum(last + level, jnp.max(end_log, axis=-1))
    keep = jnp.exp(last + level - new_level)
    fresh = jnp.exp(end_log - new_level[:, None])
    scaled_key = (fresh[:, :, None] * key).astype(jnp.bfloat16)
    new_state = keep[:, None, None] * state + jnp.einsum(
        "hse,hsd->hed", value, scaled_key, preferred_element_type=jnp.float32
    )
    new_normal = keep[:, None] * normal + jnp.sum(scaled_key.astype(jnp.float32), axis=1)
    return ((new_state, new_normal, new_level), result)


def depthwise(extended, kernel):
    taps = kernel.shape[0]
    length = extended.shape[0] - taps + 1
    total = extended[0:length] * kernel[0]
    for index in range(1, taps):
        total = total + extended[index : index + length] * kernel[index]
    return total


def merge_states(first, second):
    first_state, first_normal, first_level, first_total = first
    second_state, second_normal, second_level, second_total = second
    shifted = first_level + second_total
    level = jnp.maximum(shifted, second_level)
    older = jnp.exp(shifted - level)
    newer = jnp.exp(second_level - level)
    state = older[:, None, None] * first_state + newer[:, None, None] * second_state
    normal = older[:, None] * first_normal + newer[:, None] * second_normal
    return (state, normal, level, first_total + second_total)


def on_device_by_position(
    tokens,
    conv_value_weight,
    conv_gate_weight,
    conv_kernel,
    conv_norm_gain,
    query_weight,
    key_weight,
    value_weight,
    input_gate_weight,
    forget_gate_weight,
    input_offset,
    forget_offset,
    memory_norm_gain,
    conv_out_weight,
    memory_out_weight,
):
    length = tokens.shape[0]
    heads_here = input_gate_weight.shape[1]
    whole = lax.all_gather(tokens, "tp", axis=1, tiled=True)
    pieces = (
        lax.all_gather(conv_value_weight, "sp", axis=0, tiled=True),
        lax.all_gather(conv_gate_weight, "sp", axis=0, tiled=True),
        lax.all_gather(query_weight, "sp", axis=0, tiled=True),
        lax.all_gather(key_weight, "sp", axis=0, tiled=True),
        lax.all_gather(value_weight, "sp", axis=0, tiled=True),
    )
    folded = tuple((jnp.dot(whole, piece, preferred_element_type=jnp.float32) for piece in pieces))
    conv_value, conv_gate, query_flat, key_flat, value_flat = folded
    gate_pre = jnp.dot(whole, input_gate_weight, preferred_element_type=jnp.float32)
    forget_pre = jnp.dot(whole, forget_gate_weight, preferred_element_type=jnp.float32)
    glu = (conv_value * jax.nn.sigmoid(conv_gate)).astype(jnp.bfloat16)
    taps = conv_kernel.shape[0]
    head_dim = query_flat.shape[1] // heads_here

    def to_heads(flat):
        return flat.astype(jnp.bfloat16).reshape(length, heads_here, head_dim).transpose(1, 0, 2)

    query = to_heads(query_flat)
    key = to_heads(key_flat)
    value = to_heads(value_flat)
    gate_in = (gate_pre + input_offset).T
    forget_log = jax.nn.log_sigmoid(forget_pre + forget_offset).T
    within = jnp.cumsum(forget_log, axis=1)
    total = within[:, -1]
    end_log = total[:, None] - within + gate_in
    local_level = jnp.max(end_log, axis=1)
    fresh = jnp.exp(end_log - local_level[:, None])
    scaled_key = (fresh[:, :, None] * key).astype(jnp.bfloat16)
    local_state = jnp.einsum("hse,hsd->hed", value, scaled_key, preferred_element_type=jnp.float32)
    local_normal = jnp.sum(scaled_key.astype(jnp.float32), axis=1)
    blank_state = (
        jnp.zeros_like(local_state),
        jnp.zeros_like(local_normal),
        jnp.full_like(local_level, LOWEST_LEVEL),
        jnp.zeros_like(total),
    )
    prior = shifted_2(glu[length - (taps - 1) :], "sp", 1)
    incoming = carried_in(
        (local_state, local_normal, local_level, total), "sp", merge_states, blank_state
    )
    extended = jnp.concatenate([prior, glu], axis=0).astype(jnp.float32)
    conv = depthwise(extended, conv_kernel.astype(jnp.float32))
    blocks = length // BLOCK

    def split(array):
        return jnp.moveaxis(array.reshape((heads_here, blocks, BLOCK) + array.shape[2:]), 1, 0)

    _, hidden = lax.scan(
        block_step,
        tuple(incoming[:3]),
        (split(query), split(key), split(value), split(gate_in), split(forget_log)),
    )
    hidden = jnp.moveaxis(hidden, 0, 1).reshape(heads_here, length, head_dim)
    hidden_squares = jnp.sum(hidden * hidden, axis=(0, 2))
    channel_sum, channel_squares, memory_squares = lax.psum(
        (jnp.sum(conv, axis=1), jnp.sum(conv * conv, axis=1), hidden_squares), "tp"
    )
    channels = conv.shape[1] * lax.axis_size("tp")
    mean = (channel_sum / channels)[:, None]
    variance = (channel_squares / channels)[:, None] - mean * mean
    conv_branch = jax.nn.silu((conv - mean) * lax.rsqrt(variance + EPS) * conv_norm_gain).astype(
        jnp.bfloat16
    )
    entries = heads_here * head_dim * lax.axis_size("tp")
    memory_scale = lax.rsqrt(memory_squares / entries + EPS)
    hidden = hidden * memory_scale[None, :, None]
    hidden = hidden * memory_norm_gain.reshape(heads_here, 1, head_dim)
    memory_branch = (
        hidden.transpose(1, 0, 2).reshape(length, heads_here * head_dim).astype(jnp.bfloat16)
    )
    conv_columns, memory_columns = (
        lax.all_gather(conv_out_weight, "sp", axis=1, tiled=True),
        lax.all_gather(memory_out_weight, "sp", axis=1, tiled=True),
    )
    contract = (((0,), (1,)), ((), ()))
    summed = lax.psum_scatter(
        (
            lax.dot_general(conv_columns, conv_branch, contract, preferred_element_type=jnp.float32)
            + lax.dot_general(
                memory_columns, memory_branch, contract, preferred_element_type=jnp.float32
            )
        ).astype(jnp.bfloat16),
        "tp",
        scatter_dimension=0,
        tiled=True,
    ).astype(jnp.float32)
    return summed.T.astype(jnp.bfloat16)


def forget_parts(forget_log):
    coarse = jnp.round(forget_log * 8.0) * 0.125
    return jnp.cumsum(coarse, axis=-1), jnp.cumsum(forget_log - coarse, axis=-1)


def exchange_weights(pieces):
    return lax.all_to_all(pieces, "sp", 0, 0, tiled=False)


def gather_tokens(tokens):
    whole = lax.all_gather(tokens, "tp", axis=1, tiled=True)
    return lax.all_gather(whole, "sp", axis=0, tiled=True)


def gather_in_group(mine, size):
    count = lax.axis_size("sp")
    groups = [list(range(first, first + size)) for first in range(0, count, size)]
    return lax.all_gather(mine, "sp", axis_index_groups=groups)


def on_device_by_column(
    tokens,
    conv_value_weight,
    conv_gate_weight,
    conv_kernel,
    conv_norm_gain,
    query_weight,
    key_weight,
    value_weight,
    input_gate_weight,
    forget_gate_weight,
    input_offset,
    forget_offset,
    memory_norm_gain,
    conv_out_weight,
    memory_out_weight,
):
    f32, bf16 = jnp.float32, jnp.bfloat16
    count = lax.axis_size("sp")
    columns = lax.axis_size("tp")
    place = lax.axis_index("sp")
    heads_here = input_gate_weight.shape[1]
    size = count // heads_here
    head, quarter = place // size, place % size
    depth = query_weight.shape[0]
    head_dim = query_weight.shape[1] // heads_here
    slab = head_dim // size
    channels = conv_value_weight.shape[1] // count
    pieces = jnp.concatenate(
        [
            w.reshape(depth, count, -1)
            for w in (query_weight, key_weight, value_weight, conv_value_weight, conv_gate_weight)
        ],
        axis=2,
    ).transpose(1, 0, 2)
    weights = exchange_weights(pieces).reshape(count * depth, -1)
    whole = gather_tokens(tokens)
    length = whole.shape[0]
    offsets = lax.all_gather(
        jnp.concatenate([input_offset, forget_offset], axis=1), "sp", axis=0, tiled=True
    )
    gate_weights = jnp.concatenate([input_gate_weight, forget_gate_weight], axis=1)
    flat = jnp.dot(whole, weights, preferred_element_type=f32)
    gates = (jnp.dot(whole, gate_weights, preferred_element_type=f32) + offsets).T
    glu = (
        flat[:, 3 * slab : 3 * slab + channels] * jax.nn.sigmoid(flat[:, 3 * slab + channels :])
    ).astype(bf16)
    parts = gather_in_group(flat[:, : 3 * slab].astype(bf16), size)

    taps = conv_kernel.shape[0]
    kernel = lax.dynamic_slice_in_dim(conv_kernel, place * channels, channels, 1).astype(f32)
    extended = jnp.concatenate([jnp.zeros((taps - 1, channels), f32), glu.astype(f32)], axis=0)
    conv = depthwise(extended, kernel)

    rows = length // size
    start = quarter * rows
    gate_in = lax.dynamic_index_in_dim(gates[:heads_here], head, 0, False)
    forget_log = jax.nn.log_sigmoid(
        lax.dynamic_index_in_dim(gates[heads_here:], head, 0, False)
    )
    coarse, fine = forget_parts(forget_log)
    mine_coarse = lax.dynamic_slice_in_dim(coarse, start, rows)
    mine_fine = lax.dynamic_slice_in_dim(fine, start, rows)
    log_weight = (
        (mine_coarse[:, None] - coarse[None, :])
        + (mine_fine[:, None] - fine[None, :])
        + gate_in[None, :]
    )
    causal = (start + jnp.arange(rows))[:, None] >= jnp.arange(length)[None, :]
    log_weight = jnp.where(causal, log_weight, -jnp.inf)
    weight = jnp.exp(log_weight - jnp.max(log_weight, axis=1, keepdims=True))
    query = lax.dynamic_slice_in_dim(parts[:, :, :slab], start, rows, 1)
    query = query.transpose(1, 0, 2).reshape(rows, head_dim)
    key = parts[:, :, slab : 2 * slab].transpose(1, 0, 2).reshape(length, head_dim)
    value = parts[:, :, 2 * slab :].transpose(1, 0, 2).reshape(length, head_dim)
    scores = jnp.einsum("td,sd->ts", query, key, preferred_element_type=f32) * (
        weight * head_dim ** (-0.5)
    )
    numer = jnp.dot(scores.astype(bf16), value, preferred_element_type=f32)
    denom = jnp.sum(scores, axis=1)
    cell = numer / jnp.maximum(jnp.abs(denom), 1.0)[:, None]

    squares = lax.dynamic_update_slice_in_dim(
        jnp.zeros((length,), f32), jnp.sum(cell * cell, axis=1), start, 0
    )
    sums = lax.psum(
        jnp.stack([jnp.sum(conv, axis=1), jnp.sum(conv * conv, axis=1), squares]), ("sp", "tp")
    )
    total = channels * count * columns
    mean = sums[0] / total
    variance = sums[1] / total - mean * mean
    gain = lax.dynamic_slice_in_dim(conv_norm_gain, place * channels, channels)
    conv_branch = jax.nn.silu(
        (conv - mean[:, None]) * lax.rsqrt(variance + EPS)[:, None] * gain
    ).astype(bf16)
    entries = heads_here * head_dim * columns
    memory_scale = lax.rsqrt(lax.dynamic_slice_in_dim(sums[2], start, rows) / entries + EPS)
    memory_gain = lax.dynamic_slice_in_dim(memory_norm_gain, head * head_dim, head_dim)
    memory_branch = (cell * memory_scale[:, None] * memory_gain).astype(bf16)

    conv_all = lax.all_gather(conv_branch, "sp")
    memory_all = lax.all_gather(memory_branch, "sp")
    conv_all = conv_all.transpose(1, 0, 2).reshape(length, -1)
    memory_all = (
        memory_all.reshape(heads_here, length, head_dim).transpose(1, 0, 2).reshape(length, -1)
    )
    partial = (
        jnp.dot(conv_all, conv_out_weight, preferred_element_type=f32)
        + jnp.dot(memory_all, memory_out_weight, preferred_element_type=f32)
    ).astype(bf16)
    return send_partials(partial)


def send_partials(partial):
    count, columns = lax.axis_size("sp"), lax.axis_size("tp")
    length, width = partial.shape
    swapped = lax.all_to_all(partial.reshape(count, length // count, width), "sp", 0, 0)
    swapped = swapped.reshape(columns, count // columns, length // count, width)
    groups = lax.all_to_all(swapped, "tp", 0, 0)
    summed = jnp.sum(groups.astype(jnp.float32), axis=0).astype(jnp.bfloat16)
    return summed.transpose(1, 0, 2).reshape(length // count, -1)


def splits_by_column(mesh, tokens, query_weight, conv_value_weight, input_gate_weight):
    count, columns = mesh.shape["sp"], mesh.shape["tp"]
    heads_here = input_gate_weight.shape[1] // columns
    head_dim = query_weight.shape[1] // input_gate_weight.shape[1]
    if count % heads_here or count % columns:
        return False
    size = count // heads_here
    return (
        tokens.size * 2 <= 8 * 2**20
        and head_dim % size == 0
        and tokens.shape[0] % (size * 8) == 0
        and conv_value_weight.shape[1] % (count * columns) == 0
    )


def solution(mesh):
    in_specs = (
        P("sp", "tp"),
        P("sp", "tp"),
        P("sp", "tp"),
        P(None, "tp"),
        P("tp"),
        P("sp", "tp"),
        P("sp", "tp"),
        P("sp", "tp"),
        P(None, "tp"),
        P(None, "tp"),
        P("sp", "tp"),
        P("sp", "tp"),
        P("tp"),
        P("tp", "sp"),
        P("tp", "sp"),
    )
    out_specs = P("sp", "tp")

    def run(*arrays):
        by_column = splits_by_column(mesh, arrays[0], arrays[5], arrays[1], arrays[8])
        on_device = on_device_by_column if by_column else on_device_by_position
        return jax.shard_map(
            on_device, mesh=mesh, in_specs=in_specs, out_specs=out_specs, check_vma=False
        )(*arrays)

    return run
```

```python
import jax
import jax.numpy as jnp
from jax import lax
from jax.experimental import pallas as pl
from jax.experimental.pallas import tpu as pltpu
from jax.sharding import PartitionSpec as P

BLOCK = 64


EPS = 1e-06
LOWEST_LEVEL = -1e30


def shifted_2(value, axis, steps):
    count = lax.axis_size(axis)
    leading, last = (max(0, -steps), min(count, count - steps))
    return lax.ppermute(value, axis, [(source, source + steps) for source in range(leading, last)])


def carried_in(shard, axis, join, neutral):
    place = lax.axis_index(axis)
    gathered = jax.tree.map(
        lambda a, kind: lax.all_gather(a.astype(kind), axis),
        shard,
        (jnp.bfloat16, jnp.bfloat16, jnp.bfloat16, jnp.bfloat16),
    )
    state = jax.tree.map(lambda a, e: jnp.zeros_like(a) + jnp.asarray(e, a.dtype), shard, neutral)

    def one(step, state):
        return join(
            state,
            jax.tree.map(
                lambda a, own: lax.dynamic_index_in_dim(a, step, 0, False).astype(own.dtype),
                gathered,
                shard,
            ),
        )

    return lax.fori_loop(0, place, one, state)


def block_step(carry, inputs):
    state, normal, level = carry
    query, key, value, gate_in, forget_log = inputs
    length = gate_in.shape[-1]
    scale = query.shape[-1] ** (-0.5)
    causal = jnp.tril(jnp.ones((length, length), dtype=bool))
    within = jnp.cumsum(forget_log, axis=-1)
    log_weight = within[:, :, None] - within[:, None, :] + gate_in[:, None, :]
    log_weight = jnp.where(causal, log_weight, -jnp.inf)
    carried = within + level[:, None]
    top = jnp.maximum(carried, jnp.max(log_weight, axis=-1))
    weight = jnp.exp(log_weight - top[:, :, None])
    carried_weight = jnp.exp(carried - top) * scale
    scores = jnp.einsum("htd,hsd->hts", query, key, preferred_element_type=jnp.float32) * (
        scale * weight
    )
    numer = jnp.einsum(
        "hts,hse->hte", scores.astype(jnp.bfloat16), value, preferred_element_type=jnp.float32
    )
    numer = numer + carried_weight[:, :, None] * jnp.einsum(
        "hed,htd->hte", state.astype(jnp.bfloat16), query, preferred_element_type=jnp.float32
    )
    denom = jnp.sum(scores, axis=-1) + carried_weight * jnp.einsum(
        "hd,htd->ht", normal.astype(jnp.bfloat16), query, preferred_element_type=jnp.float32
    )
    result = numer / jnp.maximum(jnp.abs(denom), 1.0)[:, :, None]
    last = within[:, -1]
    end_log = last[:, None] - within + gate_in
    new_level = jnp.maximum(last + level, jnp.max(end_log, axis=-1))
    keep = jnp.exp(last + level - new_level)
    fresh = jnp.exp(end_log - new_level[:, None])
    scaled_key = (fresh[:, :, None] * key).astype(jnp.bfloat16)
    new_state = keep[:, None, None] * state + jnp.einsum(
        "hse,hsd->hed", value, scaled_key, preferred_element_type=jnp.float32
    )
    new_normal = keep[:, None] * normal + jnp.sum(scaled_key.astype(jnp.float32), axis=1)
    return ((new_state, new_normal, new_level), result)


def depthwise(extended, kernel):
    taps = kernel.shape[0]
    length = extended.shape[0] - taps + 1
    total = extended[0:length] * kernel[0]
    for index in range(1, taps):
        total = total + extended[index : index + length] * kernel[index]
    return total


def merge_states(first, second):
    first_state, first_normal, first_level, first_total = first
    second_state, second_normal, second_level, second_total = second
    shifted = first_level + second_total
    level = jnp.maximum(shifted, second_level)
    older = jnp.exp(shifted - level)
    newer = jnp.exp(second_level - level)
    state = older[:, None, None] * first_state + newer[:, None, None] * second_state
    normal = older[:, None] * first_normal + newer[:, None] * second_normal
    return (state, normal, level, first_total + second_total)


def on_device_by_position(
    tokens,
    conv_value_weight,
    conv_gate_weight,
    conv_kernel,
    conv_norm_gain,
    query_weight,
    key_weight,
    value_weight,
    input_gate_weight,
    forget_gate_weight,
    input_offset,
    forget_offset,
    memory_norm_gain,
    conv_out_weight,
    memory_out_weight,
):
    length = tokens.shape[0]
    heads_here = input_gate_weight.shape[1]
    whole = lax.all_gather(tokens, "tp", axis=1, tiled=True)
    pieces = (
        lax.all_gather(conv_value_weight, "sp", axis=0, tiled=True),
        lax.all_gather(conv_gate_weight, "sp", axis=0, tiled=True),
        lax.all_gather(query_weight, "sp", axis=0, tiled=True),
        lax.all_gather(key_weight, "sp", axis=0, tiled=True),
        lax.all_gather(value_weight, "sp", axis=0, tiled=True),
    )
    folded = tuple((jnp.dot(whole, piece, preferred_element_type=jnp.float32) for piece in pieces))
    conv_value, conv_gate, query_flat, key_flat, value_flat = folded
    gate_pre = jnp.dot(whole, input_gate_weight, preferred_element_type=jnp.float32)
    forget_pre = jnp.dot(whole, forget_gate_weight, preferred_element_type=jnp.float32)
    glu = (conv_value * jax.nn.sigmoid(conv_gate)).astype(jnp.bfloat16)
    taps = conv_kernel.shape[0]
    head_dim = query_flat.shape[1] // heads_here

    def to_heads(flat):
        return flat.astype(jnp.bfloat16).reshape(length, heads_here, head_dim).transpose(1, 0, 2)

    query = to_heads(query_flat)
    key = to_heads(key_flat)
    value = to_heads(value_flat)
    gate_in = (gate_pre + input_offset).T
    forget_log = jax.nn.log_sigmoid(forget_pre + forget_offset).T
    within = jnp.cumsum(forget_log, axis=1)
    total = within[:, -1]
    end_log = total[:, None] - within + gate_in
    local_level = jnp.max(end_log, axis=1)
    fresh = jnp.exp(end_log - local_level[:, None])
    scaled_key = (fresh[:, :, None] * key).astype(jnp.bfloat16)
    local_state = jnp.einsum("hse,hsd->hed", value, scaled_key, preferred_element_type=jnp.float32)
    local_normal = jnp.sum(scaled_key.astype(jnp.float32), axis=1)
    blank_state = (
        jnp.zeros_like(local_state),
        jnp.zeros_like(local_normal),
        jnp.full_like(local_level, LOWEST_LEVEL),
        jnp.zeros_like(total),
    )
    prior = shifted_2(glu[length - (taps - 1) :], "sp", 1)
    incoming = carried_in(
        (local_state, local_normal, local_level, total), "sp", merge_states, blank_state
    )
    extended = jnp.concatenate([prior, glu], axis=0).astype(jnp.float32)
    conv = depthwise(extended, conv_kernel.astype(jnp.float32))
    blocks = length // BLOCK

    def split(array):
        return jnp.moveaxis(array.reshape((heads_here, blocks, BLOCK) + array.shape[2:]), 1, 0)

    _, hidden = lax.scan(
        block_step,
        tuple(incoming[:3]),
        (split(query), split(key), split(value), split(gate_in), split(forget_log)),
    )
    hidden = jnp.moveaxis(hidden, 0, 1).reshape(heads_here, length, head_dim)
    hidden_squares = jnp.sum(hidden * hidden, axis=(0, 2))
    channel_sum, channel_squares, memory_squares = lax.psum(
        (jnp.sum(conv, axis=1), jnp.sum(conv * conv, axis=1), hidden_squares), "tp"
    )
    channels = conv.shape[1] * lax.axis_size("tp")
    mean = (channel_sum / channels)[:, None]
    variance = (channel_squares / channels)[:, None] - mean * mean
    conv_branch = jax.nn.silu((conv - mean) * lax.rsqrt(variance + EPS) * conv_norm_gain).astype(
        jnp.bfloat16
    )
    entries = heads_here * head_dim * lax.axis_size("tp")
    memory_scale = lax.rsqrt(memory_squares / entries + EPS)
    hidden = hidden * memory_scale[None, :, None]
    hidden = hidden * memory_norm_gain.reshape(heads_here, 1, head_dim)
    memory_branch = (
        hidden.transpose(1, 0, 2).reshape(length, heads_here * head_dim).astype(jnp.bfloat16)
    )
    conv_columns, memory_columns = (
        lax.all_gather(conv_out_weight, "sp", axis=1, tiled=True),
        lax.all_gather(memory_out_weight, "sp", axis=1, tiled=True),
    )
    contract = (((0,), (1,)), ((), ()))
    summed = lax.psum_scatter(
        (
            lax.dot_general(conv_columns, conv_branch, contract, preferred_element_type=jnp.float32)
            + lax.dot_general(
                memory_columns, memory_branch, contract, preferred_element_type=jnp.float32
            )
        ).astype(jnp.bfloat16),
        "tp",
        scatter_dimension=0,
        tiled=True,
    ).astype(jnp.float32)
    return summed.T.astype(jnp.bfloat16)


def forget_parts(forget_log):
    coarse = jnp.round(forget_log * 8.0) * 0.125
    return jnp.cumsum(coarse, axis=-1), jnp.cumsum(forget_log - coarse, axis=-1)


MESH = pl.DeviceIdType.MESH
IN_VMEM = pl.BlockSpec(memory_space=pltpu.VMEM)
ROLES = 4


class Sends:
    def __init__(self, semaphores):
        self.semaphores = semaphores
        self.started = []

    def start(self, source, target, arrival, device, *conditions):
        semaphore = self.semaphores.at[len(self.started)]
        copy = pltpu.make_async_remote_copy(
            src_ref=source,
            dst_ref=target,
            send_sem=semaphore,
            recv_sem=arrival,
            device_id=device,
            device_id_type=MESH,
        )
        self.started.append((copy, conditions))
        when(conditions, copy.start)

    def finish(self):
        for copy, conditions in self.started:
            when(conditions, copy.wait_send)


def when(conditions, action):
    if not conditions:
        action()
        return
    every = conditions[0]
    for condition in conditions[1:]:
        every = jnp.logical_and(every, condition)
    pl.when(every)(action)


def arrived(block, semaphore, *conditions):
    copy = pltpu.make_async_remote_copy(
        src_ref=block,
        dst_ref=block,
        send_sem=semaphore,
        recv_sem=semaphore,
        device_id=(lax.axis_index("sp"), lax.axis_index("tp")),
        device_id_type=MESH,
    )
    when(conditions, copy.wait_recv)


def line_order(here, count):
    order = []
    for distance in range(1, count):
        order.append((here - distance, here >= distance, here + 1, here + 1 < count))
        order.append((here + distance, here + distance < count, here - 1, here > 0))
    return order


def project_kernel(
    count,
    columns,
    tokens,
    wq,
    wk,
    wv,
    wcv,
    wcg,
    gate_weights,
    flat,
    gates,
    query,
    key,
    value,
    whole,
    weights,
    mine,
    send_sem,
    token_sem,
    weight_sem,
    half_sem,
    group_sem,
):
    me, tp = lax.axis_index("sp"), lax.axis_index("tp")
    layers = count // 2
    z, x, y, core = me // 2, lax.rem(me, 2), tp // 2, lax.rem(tp, 2)
    length, features = tokens.shape
    depth = wq.shape[0]
    wide = weights.shape[1]
    narrow = wide // 2
    barrier = pltpu.get_barrier_semaphore()
    y_side, core_side = (1 - y) * 2 + core, y * 2 + 1 - core
    for step in range(1, count):
        pl.semaphore_signal(
            barrier, inc=1, device_id=(lax.rem(me + step, count), tp), device_id_type=MESH
        )
    for side in (y_side, core_side):
        pl.semaphore_signal(barrier, inc=1, device_id=(me, side), device_id_type=MESH)

    def block(i, j):
        return whole.at[
            pl.ds(pl.multiple_of(i * length, length), length),
            pl.ds(pl.multiple_of(j * features, features), features),
        ]

    whole[
        pl.ds(pl.multiple_of(me * length, length), length),
        pl.ds(pl.multiple_of(tp * features, features), features),
    ] = tokens[...]
    sends = Sends(send_sem)
    rows = pl.ds(pl.multiple_of(me * depth, depth), depth)
    pl.semaphore_wait(barrier, count + 1)

    def pass_on(i, j, source, sides, *conditions):
        for device in sides:
            sends.start(source, block(i, j), token_sem.at[i, j], device, *conditions)

    x_side = z * 2 + 1 - x
    sends.start(tokens, block(me, tp), token_sem.at[me, tp], (me - 2, tp), z > 0)
    sends.start(tokens, block(me, tp), token_sem.at[me, tp], (me + 2, tp), z + 1 < layers)
    pass_on(me, tp, tokens, ((x_side, tp), (me, y_side), (me, core_side)))
    for target in range(count):
        head, role = target // ROLES, target % ROLES
        away = me != target
        if role < 3:
            window = (wq, wk, wv)[role].at[:, head * wide : (head + 1) * wide]
            sends.start(window, weights.at[rows, :], weight_sem.at[me], (target, tp), away)

            @pl.when(me == target)
            def _():
                weights[rows, :] = window[...]
        else:
            for side, (source, semaphore) in enumerate(((wcv, weight_sem), (wcg, half_sem))):
                window = source.at[:, head * narrow : (head + 1) * narrow]
                place = weights.at[rows, side * narrow : (side + 1) * narrow]
                sends.start(window, place, semaphore.at[me], (target, tp), away)

                @pl.when(me == target)
                def _():
                    place[...] = window[...]

    order = line_order(z, layers)
    for source, there, onward, further in order:
        i = source * 2 + x
        arrived(block(i, tp), token_sem.at[i, tp], there)
        sends.start(
            block(i, tp), block(i, tp), token_sem.at[i, tp], (onward * 2 + x, tp), there, further
        )
        pass_on(i, tp, block(i, tp), ((x_side, tp), (me, y_side), (me, core_side)), there)
    for source, there in [(z, None)] + [entry[:2] for entry in order]:
        conditions = () if there is None else (there,)
        i = source * 2 + 1 - x
        arrived(block(i, tp), token_sem.at[i, tp], *conditions)
        pass_on(i, tp, block(i, tp), ((me, y_side), (me, core_side)), *conditions)
    for step in range(count):
        i = lax.rem(me + step, count)
        arrived(block(i, y_side), token_sem.at[i, y_side])
        pass_on(i, y_side, block(i, y_side), ((me, core_side),))
    for step in range(count):
        i = lax.rem(me + step, count)
        for j in (core_side, (1 - y) * 2 + 1 - core):
            arrived(block(i, j), token_sem.at[i, j])
    role_here = lax.rem(me, ROLES)
    for step in range(1, count):
        i = lax.rem(me + step, count)
        part = pl.ds(pl.multiple_of(i * depth, depth), depth)
        arrived(weights.at[part, :], weight_sem.at[i], role_here < 3)
        arrived(weights.at[part, :narrow], weight_sem.at[i], role_here == 3)
        arrived(weights.at[part, narrow:], half_sem.at[i], role_here == 3)

    total = flat.shape[0]
    chunk = total // ROLES
    for index in range(ROLES):
        part = slice(index * chunk, (index + 1) * chunk)
        lines = whole[part, :]
        product = jnp.dot(lines, weights[...], preferred_element_type=jnp.float32)
        flat[part, :] = product
        mine[part, :] = product.astype(jnp.bfloat16)
        gates[part, :] = jnp.dot(lines, gate_weights[...], preferred_element_type=jnp.float32)

    first = me - role_here
    for role in range(ROLES):
        part = slice(role * chunk, (role + 1) * chunk)
        until = slice(0, (role + 1) * chunk)
        device = (first + role, tp)
        for sender, target, source in (
            (2, value.at[until, :], mine.at[until, :]),
            (1, key.at[until, :], mine.at[until, :]),
            (0, query, mine.at[part, :]),
        ):
            if sender != role:
                sends.start(source, target, group_sem.at[sender], device, role_here == sender)
            else:

                @pl.when(role_here == role)
                def _():
                    target[...] = source[...]

        @pl.when(role_here == role)
        def _():
            if (role + 1) * chunk < total:
                rest = slice((role + 1) * chunk, total)
                key[rest, :] = jnp.zeros_like(key[rest, :])
                value[rest, :] = jnp.zeros_like(value[rest, :])

    for role in range(ROLES):
        until = slice(0, (role + 1) * chunk)
        for sender, target in ((0, query), (1, key.at[until, :]), (2, value.at[until, :])):
            if sender != role:
                arrived(target, group_sem.at[sender], role_here == role)
    sends.finish()


def project(tokens, wq, wk, wv, wcv, wcg, gate_weights, head_dim):
    count, columns = lax.axis_size("sp"), lax.axis_size("tp")
    length, features = tokens.shape
    total = length * count
    f32, bf16 = jnp.float32, jnp.bfloat16
    shape = jax.ShapeDtypeStruct
    return pl.pallas_call(
        lambda *refs: project_kernel(count, columns, *refs),
        out_shape=(
            shape((total, head_dim), f32),
            shape((total, gate_weights.shape[1]), f32),
            shape((total // ROLES, head_dim), bf16),
            shape((total, head_dim), bf16),
            shape((total, head_dim), bf16),
        ),
        in_specs=[IN_VMEM] * 7,
        out_specs=(IN_VMEM,) * 5,
        scratch_shapes=[
            pltpu.VMEM((total, features * columns), bf16),
            pltpu.VMEM((wq.shape[0] * count, head_dim), bf16),
            pltpu.VMEM((total, head_dim), bf16),
            pltpu.SemaphoreType.DMA((128,)),
            pltpu.SemaphoreType.DMA((count, columns)),
            pltpu.SemaphoreType.DMA((count,)),
            pltpu.SemaphoreType.DMA((count,)),
            pltpu.SemaphoreType.DMA((3,)),
        ],
        compiler_params=pltpu.CompilerParams(collective_id=0, has_side_effects=True),
    )(tokens, wq, wk, wv, wcv, wcg, gate_weights)


def sums_kernel(count, columns, sums, total, slots, send_sem, arrival_sem):
    me, tp = lax.axis_index("sp"), lax.axis_index("tp")
    groups = count // ROLES
    members = groups * columns
    role = lax.rem(me, ROLES)
    own = (me // ROLES) * columns + tp
    barrier = pltpu.get_barrier_semaphore()
    peers = [lax.rem(own + step, members) for step in range(1, members)]
    devices = [((peer // columns) * ROLES + role, lax.rem(peer, columns)) for peer in peers]
    for device in devices:
        pl.semaphore_signal(barrier, inc=1, device_id=device, device_id_type=MESH)
    pl.semaphore_wait(barrier, members - 1)
    sends = Sends(send_sem)
    for device in devices:
        sends.start(sums, slots.at[own], arrival_sem.at[own], device)
    slots[own] = sums[...]
    for peer in peers:
        arrived(slots.at[peer], arrival_sem.at[peer])
    result = slots[0]
    for index in range(1, members):
        result = result + slots[index]
    total[...] = result
    sends.finish()


def sum_over_group(sums):
    count, columns = lax.axis_size("sp"), lax.axis_size("tp")
    members = count // ROLES * columns
    return pl.pallas_call(
        lambda *refs: sums_kernel(count, columns, *refs),
        out_shape=jax.ShapeDtypeStruct(sums.shape, sums.dtype),
        in_specs=[IN_VMEM],
        out_specs=IN_VMEM,
        scratch_shapes=[
            pltpu.VMEM((members,) + sums.shape, sums.dtype),
            pltpu.SemaphoreType.DMA((members,)),
            pltpu.SemaphoreType.DMA((members,)),
        ],
        compiler_params=pltpu.CompilerParams(collective_id=1, has_side_effects=True),
    )(sums)


def mix_kernel(
    count,
    columns,
    memory,
    conv,
    memory_weight,
    conv_weight,
    mixed,
    memories,
    convs,
    partial,
    slots,
    send_sem,
    memory_sem,
    conv_sem,
    slot_sem,
):
    me, tp = lax.axis_index("sp"), lax.axis_index("tp")
    layers = count // 2
    z, x = me // 2, lax.rem(me, 2)
    chunk = memory.shape[0]
    share = count // columns
    barrier = pltpu.get_barrier_semaphore()
    for step in range(1, count):
        pl.semaphore_signal(
            barrier, inc=1, device_id=(lax.rem(me + step, count), tp), device_id_type=MESH
        )
    inside = me // share == tp
    for half in range(share):
        for j in range(columns):
            source = tp * share + half

            @pl.when(tp != j)
            def _():
                pl.semaphore_signal(barrier, inc=1, device_id=(source, j), device_id_type=MESH)

    @pl.when(inside)
    def _():
        pl.semaphore_wait(barrier, count - 1)

    @pl.when(jnp.logical_not(inside))
    def _():
        pl.semaphore_wait(barrier, 2 * count - 1)

    def memory_at(i):
        rows = pl.multiple_of(lax.rem(i, ROLES) * chunk, chunk)
        return memories.at[i // ROLES, pl.ds(rows, chunk), :]

    def has_conv(i):
        return lax.rem(i, ROLES) == ROLES - 1

    sends = Sends(send_sem)

    def spread(i, own, device, *conditions):
        sends.start(
            memory if own else memory_at(i), memory_at(i), memory_sem.at[i], device, *conditions
        )
        place = convs.at[i // ROLES]
        sends.start(
            conv if own else place, place, conv_sem.at[i], device, has_conv(i), *conditions
        )

    def received(i, *conditions):
        arrived(memory_at(i), memory_sem.at[i], *conditions)
        arrived(convs.at[i // ROLES], conv_sem.at[i], has_conv(i), *conditions)

    x_side = (z * 2 + 1 - x, tp)
    spread(me, True, (me - 2, tp), z > 0)
    spread(me, True, (me + 2, tp), z + 1 < layers)
    spread(me, True, x_side)
    rows_here = pl.multiple_of(lax.rem(me, ROLES) * chunk, chunk)
    memories[me // ROLES, pl.ds(rows_here, chunk), :] = memory[...]

    @pl.when(has_conv(me))
    def _():
        convs[me // ROLES] = conv[...]

    order = line_order(z, layers)
    for source, there, onward, further in order:
        i = source * 2 + x
        received(i, there)
        spread(i, False, (onward * 2 + x, tp), there, further)
        spread(i, False, x_side, there)
    received(z * 2 + 1 - x)
    for source, there, _, _ in order:
        received(source * 2 + 1 - x, there)

    groups = count // ROLES
    head_dim = memory.shape[1]
    channels = conv.shape[1]
    length = mixed.shape[0]
    for index in range(ROLES):
        part = slice(index * chunk, (index + 1) * chunk)
        total = None
        for head in range(groups):
            term = jnp.dot(
                memories[head, part, :],
                memory_weight[head * head_dim : (head + 1) * head_dim, :],
                preferred_element_type=jnp.float32,
            ) + jnp.dot(
                convs[head, part, :],
                conv_weight[head * channels : (head + 1) * channels, :],
                preferred_element_type=jnp.float32,
            )
            total = term if total is None else total + term
        partial[part, :] = total.astype(jnp.bfloat16)
        for i in range(index * chunk // length, (index + 1) * chunk // length):
            column, half = me // share, lax.rem(me, share)
            block = partial.at[i * length : (i + 1) * length, :]
            away = jnp.logical_or(i != me, tp != column)
            sends.start(block, slots.at[half, tp], slot_sem.at[half, tp], (i, column), away)

            @pl.when(jnp.logical_not(away))
            def _():
                slots[half, tp] = block[...]

    width = partial.shape[1]
    for half in range(share):
        total = None
        for j in range(columns):
            arrived(
                slots.at[half, j],
                slot_sem.at[half, j],
                jnp.logical_or(tp * share + half != me, tp != j),
            )
        for j in range(columns):
            term = slots[half, j].astype(jnp.float32)
            total = term if total is None else total + term
        mixed[:, half * width : (half + 1) * width] = total.astype(jnp.bfloat16)
    sends.finish()


def mix(memory, conv, memory_weight, conv_weight):
    count, columns = lax.axis_size("sp"), lax.axis_size("tp")
    chunk, head_dim = memory.shape
    total, channels = conv.shape
    groups, share = count // ROLES, count // columns
    width = memory_weight.shape[1]
    length = total // count
    bf16 = jnp.bfloat16
    return pl.pallas_call(
        lambda *refs: mix_kernel(count, columns, *refs),
        out_shape=jax.ShapeDtypeStruct((length, width * share), bf16),
        in_specs=[IN_VMEM] * 4,
        out_specs=IN_VMEM,
        scratch_shapes=[
            pltpu.VMEM((groups, total, head_dim), bf16),
            pltpu.VMEM((groups, total, channels), bf16),
            pltpu.VMEM((total, width), bf16),
            pltpu.VMEM((share, columns, length, width), bf16),
            pltpu.SemaphoreType.DMA((64,)),
            pltpu.SemaphoreType.DMA((count,)),
            pltpu.SemaphoreType.DMA((count,)),
            pltpu.SemaphoreType.DMA((share, columns)),
        ],
        compiler_params=pltpu.CompilerParams(collective_id=2, has_side_effects=True),
    )(memory, conv, memory_weight, conv_weight)


def on_device_by_column(
    tokens,
    conv_value_weight,
    conv_gate_weight,
    conv_kernel,
    conv_norm_gain,
    query_weight,
    key_weight,
    value_weight,
    input_gate_weight,
    forget_gate_weight,
    input_offset,
    forget_offset,
    memory_norm_gain,
    conv_out_weight,
    memory_out_weight,
):
    f32, bf16 = jnp.float32, jnp.bfloat16
    count = lax.axis_size("sp")
    columns = lax.axis_size("tp")
    place = lax.axis_index("sp")
    heads_here = input_gate_weight.shape[1]
    head, role = place // ROLES, place % ROLES
    head_dim = query_weight.shape[1] // heads_here
    channels = conv_value_weight.shape[1] // heads_here
    gate_weights = jnp.concatenate([input_gate_weight, forget_gate_weight], axis=1)
    flat, gates, query, key, value = project(
        tokens,
        query_weight,
        key_weight,
        value_weight,
        conv_value_weight,
        conv_gate_weight,
        jnp.pad(gate_weights, ((0, 0), (0, 128 - 2 * heads_here))),
        head_dim,
    )
    length = flat.shape[0]
    offsets = lax.all_gather(
        jnp.concatenate([input_offset, forget_offset], axis=1), "sp", axis=0, tiled=True
    )
    gates = (gates[:, : 2 * heads_here] + offsets).T
    glu = (flat[:, :channels] * jax.nn.sigmoid(flat[:, channels:])).astype(bf16)
    taps = conv_kernel.shape[0]
    kernel = lax.dynamic_slice_in_dim(conv_kernel, head * channels, channels, 1).astype(f32)
    extended = jnp.concatenate([jnp.zeros((taps - 1, channels), f32), glu.astype(f32)], axis=0)
    conv = depthwise(extended, kernel)

    rows = length // ROLES
    start = role * rows
    gate_in = lax.dynamic_index_in_dim(gates[:heads_here], head, 0, False)
    forget_log = jax.nn.log_sigmoid(
        lax.dynamic_index_in_dim(gates[heads_here:], head, 0, False)
    )
    coarse, fine = forget_parts(forget_log)
    mine_coarse = lax.dynamic_slice_in_dim(coarse, start, rows)
    mine_fine = lax.dynamic_slice_in_dim(fine, start, rows)
    log_weight = (
        (mine_coarse[:, None] - coarse[None, :])
        + (mine_fine[:, None] - fine[None, :])
        + gate_in[None, :]
    )
    causal = (start + jnp.arange(rows))[:, None] >= jnp.arange(length)[None, :]
    log_weight = jnp.where(causal, log_weight, -jnp.inf)
    weight = jnp.exp(log_weight - jnp.max(log_weight, axis=1, keepdims=True))
    scores = jnp.einsum("td,sd->ts", query, key, preferred_element_type=f32) * (
        weight * head_dim ** (-0.5)
    )
    numer = jnp.dot(scores.astype(bf16), value, preferred_element_type=f32)
    denom = jnp.sum(scores, axis=1)
    cell = numer / jnp.maximum(jnp.abs(denom), 1.0)[:, None]

    squares = jnp.pad(jnp.sum(cell * cell, axis=1), (0, length - rows))
    normed = role == ROLES - 1
    sums = jnp.stack(
        [
            jnp.where(normed, jnp.sum(conv, axis=1), 0.0),
            jnp.where(normed, jnp.sum(conv * conv, axis=1), 0.0),
            squares,
        ]
    )
    sums = sum_over_group(jnp.pad(sums, ((0, 5), (0, 0))))
    total = conv_norm_gain.shape[0] * columns
    mean = sums[0] / total
    variance = sums[1] / total - mean * mean
    gain = lax.dynamic_slice_in_dim(conv_norm_gain, head * channels, channels)
    conv_branch = jax.nn.silu(
        (conv - mean[:, None]) * lax.rsqrt(variance + EPS)[:, None] * gain
    ).astype(bf16)
    entries = heads_here * head_dim * columns
    memory_scale = lax.rsqrt(sums[2, :rows] / entries + EPS)
    memory_gain = lax.dynamic_slice_in_dim(memory_norm_gain, head * head_dim, head_dim)
    memory_branch = (cell * memory_scale[:, None] * memory_gain).astype(bf16)

    return mix(memory_branch, conv_branch, memory_out_weight, conv_out_weight)


def splits_by_column(mesh, tokens, query_weight, conv_value_weight, input_gate_weight):
    count, columns = mesh.shape["sp"], mesh.shape["tp"]
    heads = input_gate_weight.shape[1]
    heads_here = heads // columns
    head_dim = query_weight.shape[1] // heads
    return (
        count == ROLES * heads_here
        and columns == 4
        and count % columns == 0
        and tokens.size * 2 <= 8 * 2**20
        and tokens.shape[0] % (count * 16) == 0
        and conv_value_weight.shape[1] * 2 == head_dim * heads
        and head_dim % 256 == 0
        and 2 * heads_here <= 128
    )


def solution(mesh):
    in_specs = (
        P("sp", "tp"),
        P("sp", "tp"),
        P("sp", "tp"),
        P(None, "tp"),
        P("tp"),
        P("sp", "tp"),
        P("sp", "tp"),
        P("sp", "tp"),
        P(None, "tp"),
        P(None, "tp"),
        P("sp", "tp"),
        P("sp", "tp"),
        P("tp"),
        P("tp", "sp"),
        P("tp", "sp"),
    )
    out_specs = P("sp", "tp")

    def run(*arrays):
        by_column = splits_by_column(mesh, arrays[0], arrays[5], arrays[1], arrays[8])
        on_device = on_device_by_column if by_column else on_device_by_position
        return jax.shard_map(
            on_device, mesh=mesh, in_specs=in_specs, out_specs=out_specs, check_vma=False
        )(*arrays)

    return run
```

```python
import jax
import jax.numpy as jnp
from jax import lax
from jax.experimental import pallas as pl
from jax.experimental.pallas import tpu as pltpu
from jax.sharding import PartitionSpec as P

BLOCK = 64


EPS = 1e-06
LOWEST_LEVEL = -1e30


def shifted_2(value, axis, steps):
    count = lax.axis_size(axis)
    leading, last = (max(0, -steps), min(count, count - steps))
    return lax.ppermute(value, axis, [(source, source + steps) for source in range(leading, last)])


def carried_in(shard, axis, join, neutral):
    place = lax.axis_index(axis)
    gathered = jax.tree.map(
        lambda a, kind: lax.all_gather(a.astype(kind), axis),
        shard,
        (jnp.bfloat16, jnp.bfloat16, jnp.bfloat16, jnp.bfloat16),
    )
    state = jax.tree.map(lambda a, e: jnp.zeros_like(a) + jnp.asarray(e, a.dtype), shard, neutral)

    def one(step, state):
        return join(
            state,
            jax.tree.map(
                lambda a, own: lax.dynamic_index_in_dim(a, step, 0, False).astype(own.dtype),
                gathered,
                shard,
            ),
        )

    return lax.fori_loop(0, place, one, state)


def block_step(carry, inputs):
    state, normal, level = carry
    query, key, value, gate_in, forget_log = inputs
    length = gate_in.shape[-1]
    scale = query.shape[-1] ** (-0.5)
    causal = jnp.tril(jnp.ones((length, length), dtype=bool))
    within = jnp.cumsum(forget_log, axis=-1)
    log_weight = within[:, :, None] - within[:, None, :] + gate_in[:, None, :]
    log_weight = jnp.where(causal, log_weight, -jnp.inf)
    carried = within + level[:, None]
    top = jnp.maximum(carried, jnp.max(log_weight, axis=-1))
    weight = jnp.exp(log_weight - top[:, :, None])
    carried_weight = jnp.exp(carried - top) * scale
    scores = jnp.einsum("htd,hsd->hts", query, key, preferred_element_type=jnp.float32) * (
        scale * weight
    )
    numer = jnp.einsum(
        "hts,hse->hte", scores.astype(jnp.bfloat16), value, preferred_element_type=jnp.float32
    )
    numer = numer + carried_weight[:, :, None] * jnp.einsum(
        "hed,htd->hte", state.astype(jnp.bfloat16), query, preferred_element_type=jnp.float32
    )
    denom = jnp.sum(scores, axis=-1) + carried_weight * jnp.einsum(
        "hd,htd->ht", normal.astype(jnp.bfloat16), query, preferred_element_type=jnp.float32
    )
    result = numer / jnp.maximum(jnp.abs(denom), 1.0)[:, :, None]
    last = within[:, -1]
    end_log = last[:, None] - within + gate_in
    new_level = jnp.maximum(last + level, jnp.max(end_log, axis=-1))
    keep = jnp.exp(last + level - new_level)
    fresh = jnp.exp(end_log - new_level[:, None])
    scaled_key = (fresh[:, :, None] * key).astype(jnp.bfloat16)
    new_state = keep[:, None, None] * state + jnp.einsum(
        "hse,hsd->hed", value, scaled_key, preferred_element_type=jnp.float32
    )
    new_normal = keep[:, None] * normal + jnp.sum(scaled_key.astype(jnp.float32), axis=1)
    return ((new_state, new_normal, new_level), result)


def depthwise(extended, kernel):
    taps = kernel.shape[0]
    length = extended.shape[0] - taps + 1
    total = extended[0:length] * kernel[0]
    for index in range(1, taps):
        total = total + extended[index : index + length] * kernel[index]
    return total


def merge_states(first, second):
    first_state, first_normal, first_level, first_total = first
    second_state, second_normal, second_level, second_total = second
    shifted = first_level + second_total
    level = jnp.maximum(shifted, second_level)
    older = jnp.exp(shifted - level)
    newer = jnp.exp(second_level - level)
    state = older[:, None, None] * first_state + newer[:, None, None] * second_state
    normal = older[:, None] * first_normal + newer[:, None] * second_normal
    return (state, normal, level, first_total + second_total)


def on_device_by_position(
    tokens,
    conv_value_weight,
    conv_gate_weight,
    conv_kernel,
    conv_norm_gain,
    query_weight,
    key_weight,
    value_weight,
    input_gate_weight,
    forget_gate_weight,
    input_offset,
    forget_offset,
    memory_norm_gain,
    conv_out_weight,
    memory_out_weight,
):
    length = tokens.shape[0]
    heads_here = input_gate_weight.shape[1]
    whole = lax.all_gather(tokens, "tp", axis=1, tiled=True)
    pieces = (
        lax.all_gather(conv_value_weight, "sp", axis=0, tiled=True),
        lax.all_gather(conv_gate_weight, "sp", axis=0, tiled=True),
        lax.all_gather(query_weight, "sp", axis=0, tiled=True),
        lax.all_gather(key_weight, "sp", axis=0, tiled=True),
        lax.all_gather(value_weight, "sp", axis=0, tiled=True),
    )
    folded = tuple((jnp.dot(whole, piece, preferred_element_type=jnp.float32) for piece in pieces))
    conv_value, conv_gate, query_flat, key_flat, value_flat = folded
    gate_pre = jnp.dot(whole, input_gate_weight, preferred_element_type=jnp.float32)
    forget_pre = jnp.dot(whole, forget_gate_weight, preferred_element_type=jnp.float32)
    glu = (conv_value * jax.nn.sigmoid(conv_gate)).astype(jnp.bfloat16)
    taps = conv_kernel.shape[0]
    head_dim = query_flat.shape[1] // heads_here

    def to_heads(flat):
        return flat.astype(jnp.bfloat16).reshape(length, heads_here, head_dim).transpose(1, 0, 2)

    query = to_heads(query_flat)
    key = to_heads(key_flat)
    value = to_heads(value_flat)
    gate_in = (gate_pre + input_offset).T
    forget_log = jax.nn.log_sigmoid(forget_pre + forget_offset).T
    within = jnp.cumsum(forget_log, axis=1)
    total = within[:, -1]
    end_log = total[:, None] - within + gate_in
    local_level = jnp.max(end_log, axis=1)
    fresh = jnp.exp(end_log - local_level[:, None])
    scaled_key = (fresh[:, :, None] * key).astype(jnp.bfloat16)
    local_state = jnp.einsum("hse,hsd->hed", value, scaled_key, preferred_element_type=jnp.float32)
    local_normal = jnp.sum(scaled_key.astype(jnp.float32), axis=1)
    blank_state = (
        jnp.zeros_like(local_state),
        jnp.zeros_like(local_normal),
        jnp.full_like(local_level, LOWEST_LEVEL),
        jnp.zeros_like(total),
    )
    prior = shifted_2(glu[length - (taps - 1) :], "sp", 1)
    incoming = carried_in(
        (local_state, local_normal, local_level, total), "sp", merge_states, blank_state
    )
    extended = jnp.concatenate([prior, glu], axis=0).astype(jnp.float32)
    conv = depthwise(extended, conv_kernel.astype(jnp.float32))
    blocks = length // BLOCK

    def split(array):
        return jnp.moveaxis(array.reshape((heads_here, blocks, BLOCK) + array.shape[2:]), 1, 0)

    _, hidden = lax.scan(
        block_step,
        tuple(incoming[:3]),
        (split(query), split(key), split(value), split(gate_in), split(forget_log)),
    )
    hidden = jnp.moveaxis(hidden, 0, 1).reshape(heads_here, length, head_dim)
    hidden_squares = jnp.sum(hidden * hidden, axis=(0, 2))
    channel_sum, channel_squares, memory_squares = lax.psum(
        (jnp.sum(conv, axis=1), jnp.sum(conv * conv, axis=1), hidden_squares), "tp"
    )
    channels = conv.shape[1] * lax.axis_size("tp")
    mean = (channel_sum / channels)[:, None]
    variance = (channel_squares / channels)[:, None] - mean * mean
    conv_branch = jax.nn.silu((conv - mean) * lax.rsqrt(variance + EPS) * conv_norm_gain).astype(
        jnp.bfloat16
    )
    entries = heads_here * head_dim * lax.axis_size("tp")
    memory_scale = lax.rsqrt(memory_squares / entries + EPS)
    hidden = hidden * memory_scale[None, :, None]
    hidden = hidden * memory_norm_gain.reshape(heads_here, 1, head_dim)
    memory_branch = (
        hidden.transpose(1, 0, 2).reshape(length, heads_here * head_dim).astype(jnp.bfloat16)
    )
    conv_columns, memory_columns = (
        lax.all_gather(conv_out_weight, "sp", axis=1, tiled=True),
        lax.all_gather(memory_out_weight, "sp", axis=1, tiled=True),
    )
    contract = (((0,), (1,)), ((), ()))
    summed = lax.psum_scatter(
        (
            lax.dot_general(conv_columns, conv_branch, contract, preferred_element_type=jnp.float32)
            + lax.dot_general(
                memory_columns, memory_branch, contract, preferred_element_type=jnp.float32
            )
        ).astype(jnp.bfloat16),
        "tp",
        scatter_dimension=0,
        tiled=True,
    ).astype(jnp.float32)
    return summed.T.astype(jnp.bfloat16)


def forget_parts(forget_log):
    coarse = jnp.round(forget_log * 8.0) * 0.125
    return jnp.cumsum(coarse, axis=-1), jnp.cumsum(forget_log - coarse, axis=-1)


MESH = pl.DeviceIdType.MESH
IN_VMEM = pl.BlockSpec(memory_space=pltpu.VMEM)
ROLES = 4


class Sends:
    def __init__(self, semaphores):
        self.semaphores = semaphores
        self.started = []

    def start(self, source, target, arrival, device, *conditions):
        semaphore = self.semaphores.at[len(self.started)]
        copy = pltpu.make_async_remote_copy(
            src_ref=source,
            dst_ref=target,
            send_sem=semaphore,
            recv_sem=arrival,
            device_id=device,
            device_id_type=MESH,
        )
        self.started.append((copy, conditions))
        when(conditions, copy.start)

    def finish(self):
        for copy, conditions in self.started:
            when(conditions, copy.wait_send)


def when(conditions, action):
    if not conditions:
        action()
        return
    every = conditions[0]
    for condition in conditions[1:]:
        every = jnp.logical_and(every, condition)
    pl.when(every)(action)


def arrived(block, semaphore, *conditions):
    copy = pltpu.make_async_remote_copy(
        src_ref=block,
        dst_ref=block,
        send_sem=semaphore,
        recv_sem=semaphore,
        device_id=(lax.axis_index("sp"), lax.axis_index("tp")),
        device_id_type=MESH,
    )
    when(conditions, copy.wait_recv)


def role_of(i):
    flip = lax.rem(i // ROLES, 2)
    return lax.rem(i, ROLES) + flip * (1 - 2 * lax.rem(i, 2))


def line_order(here, count):
    order = []
    for distance in range(1, count):
        order.append((here - distance, here >= distance, here + 1, here + 1 < count))
        order.append((here + distance, here + distance < count, here - 1, here > 0))
    return order


def project_kernel(
    count,
    columns,
    tokens,
    wq,
    wk,
    wv,
    wcv,
    wcg,
    gate_weights,
    own_offsets,
    flat,
    gates,
    query,
    key,
    value,
    offsets,
    whole,
    weights,
    mine,
    send_sem,
    token_sem,
    weight_sem,
    half_sem,
    group_sem,
    offset_sem,
):
    me, tp = lax.axis_index("sp"), lax.axis_index("tp")
    layers = count // 2
    z, x, y, core = me // 2, lax.rem(me, 2), tp // 2, lax.rem(tp, 2)
    length, features = tokens.shape
    depth = wq.shape[0]
    wide = weights.shape[1]
    narrow = wide // 2
    barrier = pltpu.get_barrier_semaphore()
    y_side, core_side = (1 - y) * 2 + core, y * 2 + 1 - core
    for step in range(1, count):
        pl.semaphore_signal(
            barrier, inc=1, device_id=(lax.rem(me + step, count), tp), device_id_type=MESH
        )
    for side in (y_side, core_side):
        pl.semaphore_signal(barrier, inc=1, device_id=(me, side), device_id_type=MESH)

    def block(i, j):
        return whole.at[
            pl.ds(pl.multiple_of(i * length, length), length),
            pl.ds(pl.multiple_of(j * features, features), features),
        ]

    whole[
        pl.ds(pl.multiple_of(me * length, length), length),
        pl.ds(pl.multiple_of(tp * features, features), features),
    ] = tokens[...]
    sends = Sends(send_sem)
    rows = pl.ds(pl.multiple_of(me * depth, depth), depth)
    pl.semaphore_wait(barrier, count + 1)

    def pass_on(i, j, source, sides, *conditions):
        for device in sides:
            sends.start(source, block(i, j), token_sem.at[i, j], device, *conditions)

    x_side = z * 2 + 1 - x
    sends.start(tokens, block(me, tp), token_sem.at[me, tp], (me - 2, tp), z > 0)
    sends.start(tokens, block(me, tp), token_sem.at[me, tp], (me + 2, tp), z + 1 < layers)
    pass_on(me, tp, tokens, ((x_side, tp), (me, y_side), (me, core_side)))
    for step in range(1, count):
        device = (lax.rem(me + step, count), tp)
        sends.start(own_offsets, offsets.at[me], offset_sem.at[me], device)
    offsets[me] = own_offsets[...]

    def send_weights():
        for target in range(count):
            head, role = target // ROLES, (target % ROLES) ^ (target // ROLES % 2)
            away = me != target
            if role < 3:
                window = (wq, wk, wv)[role].at[:, head * wide : (head + 1) * wide]
                sends.start(window, weights.at[rows, :], weight_sem.at[me], (target, tp), away)

                @pl.when(me == target)
                def _():
                    weights[rows, :] = window[...]
            else:
                for side, (source, semaphore) in enumerate(((wcv, weight_sem), (wcg, half_sem))):
                    window = source.at[:, head * narrow : (head + 1) * narrow]
                    place = weights.at[rows, side * narrow : (side + 1) * narrow]
                    sends.start(window, place, semaphore.at[me], (target, tp), away)

                    @pl.when(me == target)
                    def _():
                        place[...] = window[...]

    order = line_order(z, layers)
    for index, (source, there, onward, further) in enumerate(order):
        if index == 2:
            send_weights()
        i = source * 2 + x
        arrived(block(i, tp), token_sem.at[i, tp], there)
        sends.start(
            block(i, tp), block(i, tp), token_sem.at[i, tp], (onward * 2 + x, tp), there, further
        )
        pass_on(i, tp, block(i, tp), ((x_side, tp), (me, y_side), (me, core_side)), there)
    for source, there in [(z, None)] + [entry[:2] for entry in order]:
        conditions = () if there is None else (there,)
        i = source * 2 + 1 - x
        arrived(block(i, tp), token_sem.at[i, tp], *conditions)
        pass_on(i, tp, block(i, tp), ((me, y_side), (me, core_side)), *conditions)
    for step in range(count):
        i = lax.rem(me + step, count)
        arrived(block(i, y_side), token_sem.at[i, y_side])
        pass_on(i, y_side, block(i, y_side), ((me, core_side),))
    for step in range(count):
        i = lax.rem(me + step, count)
        for j in (core_side, (1 - y) * 2 + 1 - core):
            arrived(block(i, j), token_sem.at[i, j])
    role_here = role_of(me)
    for step in range(1, count):
        i = lax.rem(me + step, count)
        arrived(offsets.at[i], offset_sem.at[i])
        part = pl.ds(pl.multiple_of(i * depth, depth), depth)
        arrived(weights.at[part, :], weight_sem.at[i], role_here < 3)
        arrived(weights.at[part, :narrow], weight_sem.at[i], role_here == 3)
        arrived(weights.at[part, narrow:], half_sem.at[i], role_here == 3)

    total = flat.shape[0]
    chunk = total // ROLES
    for index in range(ROLES):
        part = slice(index * chunk, (index + 1) * chunk)
        lines = whole[part, :]
        product = jnp.dot(lines, weights[...], preferred_element_type=jnp.float32)
        flat[part, :] = product
        mine[part, :] = product.astype(jnp.bfloat16)
        gates[part, :] = jnp.dot(lines, gate_weights[...], preferred_element_type=jnp.float32)

    first = me - lax.rem(me, ROLES)
    flip = lax.rem(me // ROLES, 2)
    for role in range(ROLES):
        part = slice(role * chunk, (role + 1) * chunk)
        until = slice(0, (role + 1) * chunk)
        device = (first + role + flip * (1 - 2 * (role % 2)), tp)
        for sender, target, source in (
            (2, value.at[until, :], mine.at[until, :]),
            (1, key.at[until, :], mine.at[until, :]),
            (0, query, mine.at[part, :]),
        ):
            if sender != role:
                sends.start(source, target, group_sem.at[sender], device, role_here == sender)
            else:

                @pl.when(role_here == role)
                def _():
                    target[...] = source[...]

        @pl.when(role_here == role)
        def _():
            if (role + 1) * chunk < total:
                rest = slice((role + 1) * chunk, total)
                key[rest, :] = jnp.zeros_like(key[rest, :])
                value[rest, :] = jnp.zeros_like(value[rest, :])

    for role in range(ROLES):
        until = slice(0, (role + 1) * chunk)
        for sender, target in ((0, query), (1, key.at[until, :]), (2, value.at[until, :])):
            if sender != role:
                arrived(target, group_sem.at[sender], role_here == role)
    sends.finish()


def project(tokens, wq, wk, wv, wcv, wcg, gate_weights, own_offsets, head_dim):
    count, columns = lax.axis_size("sp"), lax.axis_size("tp")
    length, features = tokens.shape
    total = length * count
    f32, bf16 = jnp.float32, jnp.bfloat16
    shape = jax.ShapeDtypeStruct
    return pl.pallas_call(
        lambda *refs: project_kernel(count, columns, *refs),
        out_shape=(
            shape((total, head_dim), f32),
            shape((total, gate_weights.shape[1]), f32),
            shape((total // ROLES, head_dim), bf16),
            shape((total, head_dim), bf16),
            shape((total, head_dim), bf16),
            shape((count,) + own_offsets.shape, f32),
        ),
        in_specs=[IN_VMEM] * 8,
        out_specs=(IN_VMEM,) * 6,
        scratch_shapes=[
            pltpu.VMEM((total, features * columns), bf16),
            pltpu.VMEM((wq.shape[0] * count, head_dim), bf16),
            pltpu.VMEM((total, head_dim), bf16),
            pltpu.SemaphoreType.DMA((128,)),
            pltpu.SemaphoreType.DMA((count, columns)),
            pltpu.SemaphoreType.DMA((count,)),
            pltpu.SemaphoreType.DMA((count,)),
            pltpu.SemaphoreType.DMA((3,)),
            pltpu.SemaphoreType.DMA((count,)),
        ],
        compiler_params=pltpu.CompilerParams(collective_id=0, has_side_effects=True),
    )(tokens, wq, wk, wv, wcv, wcg, gate_weights, own_offsets)


def sums_kernel(count, columns, sums, total, slots, send_sem, arrival_sem):
    me, tp = lax.axis_index("sp"), lax.axis_index("tp")
    groups = count // ROLES
    members = groups * columns
    role = role_of(me)
    own = (me // ROLES) * columns + tp
    barrier = pltpu.get_barrier_semaphore()
    peers = [lax.rem(own + step, members) for step in range(1, members)]
    devices = []
    for peer in peers:
        group = peer // columns
        seat = role + lax.rem(group, 2) * (1 - 2 * lax.rem(role, 2))
        devices.append((group * ROLES + seat, lax.rem(peer, columns)))
    for device in devices:
        pl.semaphore_signal(barrier, inc=1, device_id=device, device_id_type=MESH)
    pl.semaphore_wait(barrier, members - 1)
    sends = Sends(send_sem)
    for device in devices:
        sends.start(sums, slots.at[own], arrival_sem.at[own], device)
    slots[own] = sums[...]
    for peer in peers:
        arrived(slots.at[peer], arrival_sem.at[peer])
    result = slots[0]
    for index in range(1, members):
        result = result + slots[index]
    total[...] = result
    sends.finish()


def sum_over_group(sums):
    count, columns = lax.axis_size("sp"), lax.axis_size("tp")
    members = count // ROLES * columns
    return pl.pallas_call(
        lambda *refs: sums_kernel(count, columns, *refs),
        out_shape=jax.ShapeDtypeStruct(sums.shape, sums.dtype),
        in_specs=[IN_VMEM],
        out_specs=IN_VMEM,
        scratch_shapes=[
            pltpu.VMEM((members,) + sums.shape, sums.dtype),
            pltpu.SemaphoreType.DMA((members,)),
            pltpu.SemaphoreType.DMA((members,)),
        ],
        compiler_params=pltpu.CompilerParams(collective_id=1, has_side_effects=True),
    )(sums)


def mix_kernel(
    count,
    columns,
    memory,
    conv,
    memory_weight,
    conv_weight,
    mixed,
    memories,
    convs,
    partial,
    slots,
    send_sem,
    memory_sem,
    conv_sem,
    slot_sem,
):
    me, tp = lax.axis_index("sp"), lax.axis_index("tp")
    layers = count // 2
    z, x = me // 2, lax.rem(me, 2)
    chunk = memory.shape[0]
    share = count // columns
    barrier = pltpu.get_barrier_semaphore()
    for step in range(1, count):
        pl.semaphore_signal(
            barrier, inc=1, device_id=(lax.rem(me + step, count), tp), device_id_type=MESH
        )
    inside = me // share == tp
    for half in range(share):
        for j in range(columns):
            source = tp * share + half

            @pl.when(tp != j)
            def _():
                pl.semaphore_signal(barrier, inc=1, device_id=(source, j), device_id_type=MESH)

    @pl.when(inside)
    def _():
        pl.semaphore_wait(barrier, count - 1)

    @pl.when(jnp.logical_not(inside))
    def _():
        pl.semaphore_wait(barrier, 2 * count - 1)

    def memory_at(i):
        rows = pl.multiple_of(role_of(i) * chunk, chunk)
        return memories.at[i // ROLES, pl.ds(rows, chunk), :]

    def has_conv(i):
        return role_of(i) == ROLES - 1

    sends = Sends(send_sem)

    def spread(i, own, device, *conditions):
        sends.start(
            memory if own else memory_at(i), memory_at(i), memory_sem.at[i], device, *conditions
        )
        place = convs.at[i // ROLES]
        sends.start(
            conv if own else place, place, conv_sem.at[i], device, has_conv(i), *conditions
        )

    def received(i, *conditions):
        arrived(memory_at(i), memory_sem.at[i], *conditions)
        arrived(convs.at[i // ROLES], conv_sem.at[i], has_conv(i), *conditions)

    x_side = (z * 2 + 1 - x, tp)
    spread(me, True, (me - 2, tp), z > 0)
    spread(me, True, (me + 2, tp), z + 1 < layers)
    spread(me, True, x_side)
    rows_here = pl.multiple_of(role_of(me) * chunk, chunk)
    memories[me // ROLES, pl.ds(rows_here, chunk), :] = memory[...]

    @pl.when(has_conv(me))
    def _():
        convs[me // ROLES] = conv[...]

    order = line_order(z, layers)
    for source, there, onward, further in order:
        i = source * 2 + x
        received(i, there)
        spread(i, False, (onward * 2 + x, tp), there, further)
        spread(i, False, x_side, there)
    received(z * 2 + 1 - x)
    for source, there, _, _ in order:
        received(source * 2 + 1 - x, there)

    groups = count // ROLES
    head_dim = memory.shape[1]
    channels = conv.shape[1]
    length = mixed.shape[0]
    for index in range(ROLES):
        part = slice(index * chunk, (index + 1) * chunk)
        total = None
        for head in range(groups):
            term = jnp.dot(
                memories[head, part, :],
                memory_weight[head * head_dim : (head + 1) * head_dim, :],
                preferred_element_type=jnp.float32,
            ) + jnp.dot(
                convs[head, part, :],
                conv_weight[head * channels : (head + 1) * channels, :],
                preferred_element_type=jnp.float32,
            )
            total = term if total is None else total + term
        partial[part, :] = total.astype(jnp.bfloat16)
        for i in range(index * chunk // length, (index + 1) * chunk // length):
            column, half = me // share, lax.rem(me, share)
            block = partial.at[i * length : (i + 1) * length, :]
            away = jnp.logical_or(i != me, tp != column)
            sends.start(block, slots.at[half, tp], slot_sem.at[half, tp], (i, column), away)

            @pl.when(jnp.logical_not(away))
            def _():
                slots[half, tp] = block[...]

    width = partial.shape[1]
    for half in range(share):
        total = None
        for j in range(columns):
            arrived(
                slots.at[half, j],
                slot_sem.at[half, j],
                jnp.logical_or(tp * share + half != me, tp != j),
            )
        for j in range(columns):
            term = slots[half, j].astype(jnp.float32)
            total = term if total is None else total + term
        mixed[:, half * width : (half + 1) * width] = total.astype(jnp.bfloat16)
    sends.finish()


def mix(memory, conv, memory_weight, conv_weight):
    count, columns = lax.axis_size("sp"), lax.axis_size("tp")
    chunk, head_dim = memory.shape
    total, channels = conv.shape
    groups, share = count // ROLES, count // columns
    width = memory_weight.shape[1]
    length = total // count
    bf16 = jnp.bfloat16
    return pl.pallas_call(
        lambda *refs: mix_kernel(count, columns, *refs),
        out_shape=jax.ShapeDtypeStruct((length, width * share), bf16),
        in_specs=[IN_VMEM] * 4,
        out_specs=IN_VMEM,
        scratch_shapes=[
            pltpu.VMEM((groups, total, head_dim), bf16),
            pltpu.VMEM((groups, total, channels), bf16),
            pltpu.VMEM((total, width), bf16),
            pltpu.VMEM((share, columns, length, width), bf16),
            pltpu.SemaphoreType.DMA((64,)),
            pltpu.SemaphoreType.DMA((count,)),
            pltpu.SemaphoreType.DMA((count,)),
            pltpu.SemaphoreType.DMA((share, columns)),
        ],
        compiler_params=pltpu.CompilerParams(collective_id=2, has_side_effects=True),
    )(memory, conv, memory_weight, conv_weight)


def on_device_by_column(
    tokens,
    conv_value_weight,
    conv_gate_weight,
    conv_kernel,
    conv_norm_gain,
    query_weight,
    key_weight,
    value_weight,
    input_gate_weight,
    forget_gate_weight,
    input_offset,
    forget_offset,
    memory_norm_gain,
    conv_out_weight,
    memory_out_weight,
):
    f32, bf16 = jnp.float32, jnp.bfloat16
    count = lax.axis_size("sp")
    columns = lax.axis_size("tp")
    place = lax.axis_index("sp")
    heads_here = input_gate_weight.shape[1]
    head, role = place // ROLES, role_of(place)
    head_dim = query_weight.shape[1] // heads_here
    channels = conv_value_weight.shape[1] // heads_here
    gate_weights = jnp.concatenate([input_gate_weight, forget_gate_weight], axis=1)
    own_offsets = jnp.concatenate([input_offset, forget_offset], axis=1).T
    flat, gates, query, key, value, offsets = project(
        tokens,
        query_weight,
        key_weight,
        value_weight,
        conv_value_weight,
        conv_gate_weight,
        jnp.pad(gate_weights, ((0, 0), (0, 128 - 2 * heads_here))),
        jnp.pad(own_offsets, ((0, -2 * heads_here % 8), (0, 0))),
        head_dim,
    )
    length = flat.shape[0]
    offsets = offsets[:, : 2 * heads_here].transpose(1, 0, 2).reshape(2 * heads_here, length)
    gates = gates[:, : 2 * heads_here].T + offsets
    glu = (flat[:, :channels] * jax.nn.sigmoid(flat[:, channels:])).astype(bf16)
    taps = conv_kernel.shape[0]
    kernel = lax.dynamic_slice_in_dim(conv_kernel, head * channels, channels, 1).astype(f32)
    extended = jnp.concatenate([jnp.zeros((taps - 1, channels), f32), glu.astype(f32)], axis=0)
    conv = depthwise(extended, kernel)

    rows = length // ROLES
    start = role * rows
    gate_in = lax.dynamic_index_in_dim(gates[:heads_here], head, 0, False)
    forget_log = jax.nn.log_sigmoid(
        lax.dynamic_index_in_dim(gates[heads_here:], head, 0, False)
    )
    coarse, fine = forget_parts(forget_log)
    mine_coarse = lax.dynamic_slice_in_dim(coarse, start, rows)
    mine_fine = lax.dynamic_slice_in_dim(fine, start, rows)
    log_weight = (
        (mine_coarse[:, None] - coarse[None, :])
        + (mine_fine[:, None] - fine[None, :])
        + gate_in[None, :]
    )
    causal = (start + jnp.arange(rows))[:, None] >= jnp.arange(length)[None, :]
    log_weight = jnp.where(causal, log_weight, -jnp.inf)
    weight = jnp.exp(log_weight - jnp.max(log_weight, axis=1, keepdims=True))
    scores = jnp.einsum("td,sd->ts", query, key, preferred_element_type=f32) * (
        weight * head_dim ** (-0.5)
    )
    numer = jnp.dot(scores.astype(bf16), value, preferred_element_type=f32)
    denom = jnp.sum(scores, axis=1)
    cell = numer / jnp.maximum(jnp.abs(denom), 1.0)[:, None]

    squares = jnp.pad(jnp.sum(cell * cell, axis=1), (0, length - rows))
    normed = role == ROLES - 1
    sums = jnp.stack(
        [
            jnp.where(normed, jnp.sum(conv, axis=1), 0.0),
            jnp.where(normed, jnp.sum(conv * conv, axis=1), 0.0),
            squares,
        ]
    )
    sums = sum_over_group(jnp.pad(sums, ((0, 5), (0, 0))))
    total = conv_norm_gain.shape[0] * columns
    mean = sums[0] / total
    variance = sums[1] / total - mean * mean
    gain = lax.dynamic_slice_in_dim(conv_norm_gain, head * channels, channels)
    conv_branch = jax.nn.silu(
        (conv - mean[:, None]) * lax.rsqrt(variance + EPS)[:, None] * gain
    ).astype(bf16)
    entries = heads_here * head_dim * columns
    memory_scale = lax.rsqrt(sums[2, :rows] / entries + EPS)
    memory_gain = lax.dynamic_slice_in_dim(memory_norm_gain, head * head_dim, head_dim)
    memory_branch = (cell * memory_scale[:, None] * memory_gain).astype(bf16)

    return mix(memory_branch, conv_branch, memory_out_weight, conv_out_weight)


def splits_by_column(mesh, tokens, query_weight, conv_value_weight, input_gate_weight):
    count, columns = mesh.shape["sp"], mesh.shape["tp"]
    heads = input_gate_weight.shape[1]
    heads_here = heads // columns
    head_dim = query_weight.shape[1] // heads
    return (
        count == ROLES * heads_here
        and columns == 4
        and count % columns == 0
        and tokens.size * 2 <= 8 * 2**20
        and tokens.shape[0] % (count * 16) == 0
        and conv_value_weight.shape[1] * 2 == head_dim * heads
        and head_dim % 256 == 0
        and 2 * heads_here <= 128
    )


def solution(mesh):
    in_specs = (
        P("sp", "tp"),
        P("sp", "tp"),
        P("sp", "tp"),
        P(None, "tp"),
        P("tp"),
        P("sp", "tp"),
        P("sp", "tp"),
        P("sp", "tp"),
        P(None, "tp"),
        P(None, "tp"),
        P("sp", "tp"),
        P("sp", "tp"),
        P("tp"),
        P("tp", "sp"),
        P("tp", "sp"),
    )
    out_specs = P("sp", "tp")

    def run(*arrays):
        by_column = splits_by_column(mesh, arrays[0], arrays[5], arrays[1], arrays[8])
        on_device = on_device_by_column if by_column else on_device_by_position
        return jax.shard_map(
            on_device, mesh=mesh, in_specs=in_specs, out_specs=out_specs, check_vma=False
        )(*arrays)

    return run
```

```python
import jax
import jax.numpy as jnp
from jax import lax
from jax.experimental import pallas as pl
from jax.experimental.pallas import tpu as pltpu
from jax.sharding import PartitionSpec as P

BLOCK = 64


EPS = 1e-06
LOWEST_LEVEL = -1e30


def shifted_2(value, axis, steps):
    count = lax.axis_size(axis)
    leading, last = (max(0, -steps), min(count, count - steps))
    return lax.ppermute(value, axis, [(source, source + steps) for source in range(leading, last)])


def carried_in(shard, axis, join, neutral):
    place = lax.axis_index(axis)
    gathered = jax.tree.map(
        lambda a, kind: lax.all_gather(a.astype(kind), axis),
        shard,
        (jnp.bfloat16, jnp.bfloat16, jnp.bfloat16, jnp.bfloat16),
    )
    state = jax.tree.map(lambda a, e: jnp.zeros_like(a) + jnp.asarray(e, a.dtype), shard, neutral)

    def one(step, state):
        return join(
            state,
            jax.tree.map(
                lambda a, own: lax.dynamic_index_in_dim(a, step, 0, False).astype(own.dtype),
                gathered,
                shard,
            ),
        )

    return lax.fori_loop(0, place, one, state)


def block_step(carry, inputs):
    state, normal, level = carry
    query, key, value, gate_in, forget_log = inputs
    length = gate_in.shape[-1]
    scale = query.shape[-1] ** (-0.5)
    causal = jnp.tril(jnp.ones((length, length), dtype=bool))
    within = jnp.cumsum(forget_log, axis=-1)
    log_weight = within[:, :, None] - within[:, None, :] + gate_in[:, None, :]
    log_weight = jnp.where(causal, log_weight, -jnp.inf)
    carried = within + level[:, None]
    top = jnp.maximum(carried, jnp.max(log_weight, axis=-1))
    weight = jnp.exp(log_weight - top[:, :, None])
    carried_weight = jnp.exp(carried - top) * scale
    scores = jnp.einsum("htd,hsd->hts", query, key, preferred_element_type=jnp.float32) * (
        scale * weight
    )
    numer = jnp.einsum(
        "hts,hse->hte", scores.astype(jnp.bfloat16), value, preferred_element_type=jnp.float32
    )
    numer = numer + carried_weight[:, :, None] * jnp.einsum(
        "hed,htd->hte", state.astype(jnp.bfloat16), query, preferred_element_type=jnp.float32
    )
    denom = jnp.sum(scores, axis=-1) + carried_weight * jnp.einsum(
        "hd,htd->ht", normal.astype(jnp.bfloat16), query, preferred_element_type=jnp.float32
    )
    result = numer / jnp.maximum(jnp.abs(denom), 1.0)[:, :, None]
    last = within[:, -1]
    end_log = last[:, None] - within + gate_in
    new_level = jnp.maximum(last + level, jnp.max(end_log, axis=-1))
    keep = jnp.exp(last + level - new_level)
    fresh = jnp.exp(end_log - new_level[:, None])
    scaled_key = (fresh[:, :, None] * key).astype(jnp.bfloat16)
    new_state = keep[:, None, None] * state + jnp.einsum(
        "hse,hsd->hed", value, scaled_key, preferred_element_type=jnp.float32
    )
    new_normal = keep[:, None] * normal + jnp.sum(scaled_key.astype(jnp.float32), axis=1)
    return ((new_state, new_normal, new_level), result)


def depthwise(extended, kernel):
    taps = kernel.shape[0]
    length = extended.shape[0] - taps + 1
    total = extended[0:length] * kernel[0]
    for index in range(1, taps):
        total = total + extended[index : index + length] * kernel[index]
    return total


def merge_states(first, second):
    first_state, first_normal, first_level, first_total = first
    second_state, second_normal, second_level, second_total = second
    shifted = first_level + second_total
    level = jnp.maximum(shifted, second_level)
    older = jnp.exp(shifted - level)
    newer = jnp.exp(second_level - level)
    state = older[:, None, None] * first_state + newer[:, None, None] * second_state
    normal = older[:, None] * first_normal + newer[:, None] * second_normal
    return (state, normal, level, first_total + second_total)


def on_device_by_position(
    tokens,
    conv_value_weight,
    conv_gate_weight,
    conv_kernel,
    conv_norm_gain,
    query_weight,
    key_weight,
    value_weight,
    input_gate_weight,
    forget_gate_weight,
    input_offset,
    forget_offset,
    memory_norm_gain,
    conv_out_weight,
    memory_out_weight,
):
    length = tokens.shape[0]
    heads_here = input_gate_weight.shape[1]
    whole = lax.all_gather(tokens, "tp", axis=1, tiled=True)
    pieces = (
        lax.all_gather(conv_value_weight, "sp", axis=0, tiled=True),
        lax.all_gather(conv_gate_weight, "sp", axis=0, tiled=True),
        lax.all_gather(query_weight, "sp", axis=0, tiled=True),
        lax.all_gather(key_weight, "sp", axis=0, tiled=True),
        lax.all_gather(value_weight, "sp", axis=0, tiled=True),
    )
    folded = tuple((jnp.dot(whole, piece, preferred_element_type=jnp.float32) for piece in pieces))
    conv_value, conv_gate, query_flat, key_flat, value_flat = folded
    gate_pre = jnp.dot(whole, input_gate_weight, preferred_element_type=jnp.float32)
    forget_pre = jnp.dot(whole, forget_gate_weight, preferred_element_type=jnp.float32)
    glu = (conv_value * jax.nn.sigmoid(conv_gate)).astype(jnp.bfloat16)
    taps = conv_kernel.shape[0]
    head_dim = query_flat.shape[1] // heads_here

    def to_heads(flat):
        return flat.astype(jnp.bfloat16).reshape(length, heads_here, head_dim).transpose(1, 0, 2)

    query = to_heads(query_flat)
    key = to_heads(key_flat)
    value = to_heads(value_flat)
    gate_in = (gate_pre + input_offset).T
    forget_log = jax.nn.log_sigmoid(forget_pre + forget_offset).T
    within = jnp.cumsum(forget_log, axis=1)
    total = within[:, -1]
    end_log = total[:, None] - within + gate_in
    local_level = jnp.max(end_log, axis=1)
    fresh = jnp.exp(end_log - local_level[:, None])
    scaled_key = (fresh[:, :, None] * key).astype(jnp.bfloat16)
    local_state = jnp.einsum("hse,hsd->hed", value, scaled_key, preferred_element_type=jnp.float32)
    local_normal = jnp.sum(scaled_key.astype(jnp.float32), axis=1)
    blank_state = (
        jnp.zeros_like(local_state),
        jnp.zeros_like(local_normal),
        jnp.full_like(local_level, LOWEST_LEVEL),
        jnp.zeros_like(total),
    )
    prior = shifted_2(glu[length - (taps - 1) :], "sp", 1)
    incoming = carried_in(
        (local_state, local_normal, local_level, total), "sp", merge_states, blank_state
    )
    extended = jnp.concatenate([prior, glu], axis=0).astype(jnp.float32)
    conv = depthwise(extended, conv_kernel.astype(jnp.float32))
    blocks = length // BLOCK

    def split(array):
        return jnp.moveaxis(array.reshape((heads_here, blocks, BLOCK) + array.shape[2:]), 1, 0)

    _, hidden = lax.scan(
        block_step,
        tuple(incoming[:3]),
        (split(query), split(key), split(value), split(gate_in), split(forget_log)),
    )
    hidden = jnp.moveaxis(hidden, 0, 1).reshape(heads_here, length, head_dim)
    hidden_squares = jnp.sum(hidden * hidden, axis=(0, 2))
    channel_sum, channel_squares, memory_squares = lax.psum(
        (jnp.sum(conv, axis=1), jnp.sum(conv * conv, axis=1), hidden_squares), "tp"
    )
    channels = conv.shape[1] * lax.axis_size("tp")
    mean = (channel_sum / channels)[:, None]
    variance = (channel_squares / channels)[:, None] - mean * mean
    conv_branch = jax.nn.silu((conv - mean) * lax.rsqrt(variance + EPS) * conv_norm_gain).astype(
        jnp.bfloat16
    )
    entries = heads_here * head_dim * lax.axis_size("tp")
    memory_scale = lax.rsqrt(memory_squares / entries + EPS)
    hidden = hidden * memory_scale[None, :, None]
    hidden = hidden * memory_norm_gain.reshape(heads_here, 1, head_dim)
    memory_branch = (
        hidden.transpose(1, 0, 2).reshape(length, heads_here * head_dim).astype(jnp.bfloat16)
    )
    conv_columns, memory_columns = (
        lax.all_gather(conv_out_weight, "sp", axis=1, tiled=True),
        lax.all_gather(memory_out_weight, "sp", axis=1, tiled=True),
    )
    contract = (((0,), (1,)), ((), ()))
    summed = lax.psum_scatter(
        (
            lax.dot_general(conv_columns, conv_branch, contract, preferred_element_type=jnp.float32)
            + lax.dot_general(
                memory_columns, memory_branch, contract, preferred_element_type=jnp.float32
            )
        ).astype(jnp.bfloat16),
        "tp",
        scatter_dimension=0,
        tiled=True,
    ).astype(jnp.float32)
    return summed.T.astype(jnp.bfloat16)


def forget_parts(forget_log):
    coarse = jnp.round(forget_log * 8.0) * 0.125
    return jnp.cumsum(coarse, axis=-1), jnp.cumsum(forget_log - coarse, axis=-1)


MESH = pl.DeviceIdType.MESH
IN_VMEM = pl.BlockSpec(memory_space=pltpu.VMEM)
ROLES = 4


class Sends:
    def __init__(self, semaphores):
        self.semaphores = semaphores
        self.started = []

    def start(self, source, target, arrival, device, *conditions):
        semaphore = self.semaphores.at[len(self.started)]
        copy = pltpu.make_async_remote_copy(
            src_ref=source,
            dst_ref=target,
            send_sem=semaphore,
            recv_sem=arrival,
            device_id=device,
            device_id_type=MESH,
        )
        self.started.append((copy, conditions))
        when(conditions, copy.start)

    def finish(self):
        for copy, conditions in self.started:
            when(conditions, copy.wait_send)


def when(conditions, action):
    if not conditions:
        action()
        return
    every = conditions[0]
    for condition in conditions[1:]:
        every = jnp.logical_and(every, condition)
    pl.when(every)(action)


def arrived(block, semaphore, *conditions):
    copy = pltpu.make_async_remote_copy(
        src_ref=block,
        dst_ref=block,
        send_sem=semaphore,
        recv_sem=semaphore,
        device_id=(lax.axis_index("sp"), lax.axis_index("tp")),
        device_id_type=MESH,
    )
    when(conditions, copy.wait_recv)


def role_of(i):
    flip = lax.rem(i // ROLES, 2)
    return lax.rem(i, ROLES) + flip * (1 - 2 * lax.rem(i, 2))


def line_order(here, count):
    order = []
    for distance in range(1, count):
        order.append((here - distance, here >= distance, here + 1, here + 1 < count))
        order.append((here + distance, here + distance < count, here - 1, here > 0))
    return order


def project_kernel(
    count,
    columns,
    tokens,
    wq,
    wk,
    wv,
    wcv,
    wcg,
    gate_weights,
    own_offsets,
    flat,
    gates,
    query,
    key,
    value,
    offsets,
    whole,
    weights,
    mine,
    send_sem,
    token_sem,
    weight_sem,
    half_sem,
    group_sem,
    offset_sem,
):
    me, tp = lax.axis_index("sp"), lax.axis_index("tp")
    layers = count // 2
    z, x, y, core = me // 2, lax.rem(me, 2), tp // 2, lax.rem(tp, 2)
    length, features = tokens.shape
    depth = wq.shape[0]
    wide = weights.shape[1]
    narrow = wide // 2
    barrier = pltpu.get_barrier_semaphore()
    y_side, core_side = (1 - y) * 2 + core, y * 2 + 1 - core
    for step in range(1, count):
        pl.semaphore_signal(
            barrier, inc=1, device_id=(lax.rem(me + step, count), tp), device_id_type=MESH
        )
    for side in (y_side, core_side):
        pl.semaphore_signal(barrier, inc=1, device_id=(me, side), device_id_type=MESH)

    def block(i, j):
        return whole.at[
            pl.ds(pl.multiple_of(i * length, length), length),
            pl.ds(pl.multiple_of(j * features, features), features),
        ]

    whole[
        pl.ds(pl.multiple_of(me * length, length), length),
        pl.ds(pl.multiple_of(tp * features, features), features),
    ] = tokens[...]
    sends = Sends(send_sem)
    rows = pl.ds(pl.multiple_of(me * depth, depth), depth)
    pl.semaphore_wait(barrier, count + 1)

    def pass_on(i, j, source, sides, *conditions):
        for device in sides:
            sends.start(source, block(i, j), token_sem.at[i, j], device, *conditions)

    x_side = z * 2 + 1 - x
    sends.start(tokens, block(me, tp), token_sem.at[me, tp], (me - 2, tp), z > 0)
    sends.start(tokens, block(me, tp), token_sem.at[me, tp], (me + 2, tp), z + 1 < layers)
    pass_on(me, tp, tokens, ((x_side, tp), (me, y_side), (me, core_side)))
    for step in range(1, count):
        device = (lax.rem(me + step, count), tp)
        sends.start(own_offsets, offsets.at[me], offset_sem.at[me], device)
    offsets[me] = own_offsets[...]

    def send_weights():
        for step in range(1, count):
            target = lax.rem(me + step, count)
            head, role = target // ROLES, role_of(target)
            device = (target, tp)
            window = pl.ds(pl.multiple_of(head * wide, wide), wide)
            for index, source in enumerate((wq, wk, wv)):
                sends.start(
                    source.at[:, window],
                    weights.at[rows, :],
                    weight_sem.at[me],
                    device,
                    role == index,
                )
            window = pl.ds(pl.multiple_of(head * narrow, narrow), narrow)
            for side, (source, semaphore) in enumerate(((wcv, weight_sem), (wcg, half_sem))):
                place = weights.at[rows, side * narrow : (side + 1) * narrow]
                sends.start(source.at[:, window], place, semaphore.at[me], device, role == 3)

    for target in range(count):
        head, role = target // ROLES, (target % ROLES) ^ (target // ROLES % 2)

        @pl.when(me == target)
        def _():
            if role < 3:
                weights[rows, :] = (wq, wk, wv)[role][:, head * wide : (head + 1) * wide]
            else:
                weights[rows, :narrow] = wcv[:, head * narrow : (head + 1) * narrow]
                weights[rows, narrow:] = wcg[:, head * narrow : (head + 1) * narrow]

    order = line_order(z, layers)
    for index, (source, there, onward, further) in enumerate(order):
        if index == 2:
            send_weights()
        i = source * 2 + x
        arrived(block(i, tp), token_sem.at[i, tp], there)
        sends.start(
            block(i, tp), block(i, tp), token_sem.at[i, tp], (onward * 2 + x, tp), there, further
        )
        pass_on(i, tp, block(i, tp), ((x_side, tp), (me, y_side), (me, core_side)), there)
    for source, there in [(z, None)] + [entry[:2] for entry in order]:
        conditions = () if there is None else (there,)
        i = source * 2 + 1 - x
        arrived(block(i, tp), token_sem.at[i, tp], *conditions)
        pass_on(i, tp, block(i, tp), ((me, y_side), (me, core_side)), *conditions)
    for step in range(count):
        i = lax.rem(me + step, count)
        arrived(block(i, y_side), token_sem.at[i, y_side])
        pass_on(i, y_side, block(i, y_side), ((me, core_side),))
    for step in range(count):
        i = lax.rem(me + step, count)
        for j in (core_side, (1 - y) * 2 + 1 - core):
            arrived(block(i, j), token_sem.at[i, j])
    role_here = role_of(me)
    for step in range(1, count):
        i = lax.rem(me + step, count)
        arrived(offsets.at[i], offset_sem.at[i])
        part = pl.ds(pl.multiple_of(i * depth, depth), depth)
        arrived(weights.at[part, :], weight_sem.at[i], role_here < 3)
        arrived(weights.at[part, :narrow], weight_sem.at[i], role_here == 3)
        arrived(weights.at[part, narrow:], half_sem.at[i], role_here == 3)

    total = flat.shape[0]
    chunk = total // ROLES
    for index in range(ROLES):
        part = slice(index * chunk, (index + 1) * chunk)
        lines = whole[part, :]
        product = jnp.dot(lines, weights[...], preferred_element_type=jnp.float32)
        flat[part, :] = product
        mine[part, :] = product.astype(jnp.bfloat16)
        gates[part, :] = jnp.dot(lines, gate_weights[...], preferred_element_type=jnp.float32)

    first = me - lax.rem(me, ROLES)
    flip = lax.rem(me // ROLES, 2)
    for role in range(ROLES):
        part = slice(role * chunk, (role + 1) * chunk)
        until = slice(0, (role + 1) * chunk)
        device = (first + role + flip * (1 - 2 * (role % 2)), tp)
        for sender, target, source in (
            (2, value.at[until, :], mine.at[until, :]),
            (1, key.at[until, :], mine.at[until, :]),
            (0, query, mine.at[part, :]),
        ):
            if sender != role:
                sends.start(source, target, group_sem.at[sender], device, role_here == sender)
            else:

                @pl.when(role_here == role)
                def _():
                    target[...] = source[...]

        @pl.when(role_here == role)
        def _():
            if (role + 1) * chunk < total:
                rest = slice((role + 1) * chunk, total)
                key[rest, :] = jnp.zeros_like(key[rest, :])
                value[rest, :] = jnp.zeros_like(value[rest, :])

    for role in range(ROLES):
        until = slice(0, (role + 1) * chunk)
        for sender, target in ((0, query), (1, key.at[until, :]), (2, value.at[until, :])):
            if sender != role:
                arrived(target, group_sem.at[sender], role_here == role)
    sends.finish()


def project(tokens, wq, wk, wv, wcv, wcg, gate_weights, own_offsets, head_dim):
    count, columns = lax.axis_size("sp"), lax.axis_size("tp")
    length, features = tokens.shape
    total = length * count
    f32, bf16 = jnp.float32, jnp.bfloat16
    shape = jax.ShapeDtypeStruct
    return pl.pallas_call(
        lambda *refs: project_kernel(count, columns, *refs),
        out_shape=(
            shape((total, head_dim), f32),
            shape((total, gate_weights.shape[1]), f32),
            shape((total // ROLES, head_dim), bf16),
            shape((total, head_dim), bf16),
            shape((total, head_dim), bf16),
            shape((count,) + own_offsets.shape, f32),
        ),
        in_specs=[IN_VMEM] * 8,
        out_specs=(IN_VMEM,) * 6,
        scratch_shapes=[
            pltpu.VMEM((total, features * columns), bf16),
            pltpu.VMEM((wq.shape[0] * count, head_dim), bf16),
            pltpu.VMEM((total, head_dim), bf16),
            pltpu.SemaphoreType.DMA((192,)),
            pltpu.SemaphoreType.DMA((count, columns)),
            pltpu.SemaphoreType.DMA((count,)),
            pltpu.SemaphoreType.DMA((count,)),
            pltpu.SemaphoreType.DMA((3,)),
            pltpu.SemaphoreType.DMA((count,)),
        ],
        compiler_params=pltpu.CompilerParams(collective_id=0, has_side_effects=True),
    )(tokens, wq, wk, wv, wcv, wcg, gate_weights, own_offsets)


def sums_kernel(count, columns, sums, total, slots, send_sem, arrival_sem):
    me, tp = lax.axis_index("sp"), lax.axis_index("tp")
    groups = count // ROLES
    members = groups * columns
    role = role_of(me)
    own = (me // ROLES) * columns + tp
    barrier = pltpu.get_barrier_semaphore()
    peers = [lax.rem(own + step, members) for step in range(1, members)]
    devices = []
    for peer in peers:
        group = peer // columns
        seat = role + lax.rem(group, 2) * (1 - 2 * lax.rem(role, 2))
        devices.append((group * ROLES + seat, lax.rem(peer, columns)))
    for device in devices:
        pl.semaphore_signal(barrier, inc=1, device_id=device, device_id_type=MESH)
    pl.semaphore_wait(barrier, members - 1)
    sends = Sends(send_sem)
    for device in devices:
        sends.start(sums, slots.at[own], arrival_sem.at[own], device)
    slots[own] = sums[...]
    for peer in peers:
        arrived(slots.at[peer], arrival_sem.at[peer])
    result = slots[0]
    for index in range(1, members):
        result = result + slots[index]
    total[...] = result
    sends.finish()


def sum_over_group(sums):
    count, columns = lax.axis_size("sp"), lax.axis_size("tp")
    members = count // ROLES * columns
    return pl.pallas_call(
        lambda *refs: sums_kernel(count, columns, *refs),
        out_shape=jax.ShapeDtypeStruct(sums.shape, sums.dtype),
        in_specs=[IN_VMEM],
        out_specs=IN_VMEM,
        scratch_shapes=[
            pltpu.VMEM((members,) + sums.shape, sums.dtype),
            pltpu.SemaphoreType.DMA((members,)),
            pltpu.SemaphoreType.DMA((members,)),
        ],
        compiler_params=pltpu.CompilerParams(collective_id=1, has_side_effects=True),
    )(sums)


def mix_kernel(
    count,
    columns,
    memory,
    conv,
    memory_weight,
    conv_weight,
    mixed,
    memories,
    convs,
    partial,
    slots,
    send_sem,
    memory_sem,
    conv_sem,
    slot_sem,
):
    me, tp = lax.axis_index("sp"), lax.axis_index("tp")
    layers = count // 2
    z, x = me // 2, lax.rem(me, 2)
    chunk = memory.shape[0]
    share = count // columns
    barrier = pltpu.get_barrier_semaphore()
    for step in range(1, count):
        pl.semaphore_signal(
            barrier, inc=1, device_id=(lax.rem(me + step, count), tp), device_id_type=MESH
        )
    inside = me // share == tp
    for half in range(share):
        for j in range(columns):
            source = tp * share + half

            @pl.when(tp != j)
            def _():
                pl.semaphore_signal(barrier, inc=1, device_id=(source, j), device_id_type=MESH)

    @pl.when(inside)
    def _():
        pl.semaphore_wait(barrier, count - 1)

    @pl.when(jnp.logical_not(inside))
    def _():
        pl.semaphore_wait(barrier, 2 * count - 1)

    def memory_at(i):
        rows = pl.multiple_of(role_of(i) * chunk, chunk)
        return memories.at[i // ROLES, pl.ds(rows, chunk), :]

    def has_conv(i):
        return role_of(i) == ROLES - 1

    sends = Sends(send_sem)

    def piece(index):
        return slice(index * chunk, (index + 1) * chunk)

    def spread_memory(i, own, device, *conditions):
        sends.start(
            memory if own else memory_at(i), memory_at(i), memory_sem.at[i], device, *conditions
        )

    def spread_conv(i, index, own, device, *conditions):
        place = convs.at[i // ROLES, piece(index), :]
        sends.start(
            conv.at[piece(index), :] if own else place,
            place,
            conv_sem.at[i, index],
            device,
            has_conv(i),
            *conditions,
        )

    def conv_arrived(i, index, *conditions):
        place = convs.at[i // ROLES, piece(index), :]
        arrived(place, conv_sem.at[i, index], has_conv(i), *conditions)

    x_side = (z * 2 + 1 - x, tp)
    below, above = (me - 2, tp), (me + 2, tp)
    spread_memory(me, True, below, z > 0)
    spread_memory(me, True, above, z + 1 < layers)
    spread_memory(me, True, x_side)
    for index in range(ROLES):
        spread_conv(me, index, True, below, z > 0)
        spread_conv(me, index, True, above, z + 1 < layers)
        spread_conv(me, index, True, x_side)
    rows_here = pl.multiple_of(role_of(me) * chunk, chunk)
    memories[me // ROLES, pl.ds(rows_here, chunk), :] = memory[...]

    @pl.when(has_conv(me))
    def _():
        convs[me // ROLES] = conv[...]

    order = line_order(z, layers)
    for source, there, onward, further in order:
        i = source * 2 + x
        arrived(memory_at(i), memory_sem.at[i], there)
        spread_memory(i, False, (onward * 2 + x, tp), there, further)
        spread_memory(i, False, x_side, there)
    for source, there, onward, further in order:
        i = source * 2 + x
        for index in range(ROLES):
            conv_arrived(i, index, there)
            spread_conv(i, index, False, (onward * 2 + x, tp), there, further)
            spread_conv(i, index, False, x_side, there)
    for source, there in [(z, z >= 0)] + [entry[:2] for entry in order]:
        i = source * 2 + 1 - x
        arrived(memory_at(i), memory_sem.at[i], there)
        for index in range(ROLES):
            conv_arrived(i, index, there)

    groups = count // ROLES
    head_dim = memory.shape[1]
    channels = conv.shape[1]
    length = mixed.shape[0]
    for index in range(ROLES):
        part = slice(index * chunk, (index + 1) * chunk)
        total = None
        for head in range(groups):
            term = jnp.dot(
                memories[head, part, :],
                memory_weight[head * head_dim : (head + 1) * head_dim, :],
                preferred_element_type=jnp.float32,
            ) + jnp.dot(
                convs[head, part, :],
                conv_weight[head * channels : (head + 1) * channels, :],
                preferred_element_type=jnp.float32,
            )
            total = term if total is None else total + term
        partial[part, :] = total.astype(jnp.bfloat16)
    column, half = me // share, lax.rem(me, share)
    for step in range(count):
        i = lax.rem(me + step, count)
        place = pl.ds(pl.multiple_of(i * length, length), length)
        away = jnp.logical_or(i != me, tp != column)
        sends.start(
            partial.at[place, :], slots.at[half, tp], slot_sem.at[half, tp], (i, column), away
        )
        if step == 0:

            @pl.when(jnp.logical_not(away))
            def _():
                slots[half, tp] = partial[place, :]

    width = partial.shape[1]
    for half in range(share):
        total = None
        for j in range(columns):
            arrived(
                slots.at[half, j],
                slot_sem.at[half, j],
                jnp.logical_or(tp * share + half != me, tp != j),
            )
        for j in range(columns):
            term = slots[half, j].astype(jnp.float32)
            total = term if total is None else total + term
        mixed[:, half * width : (half + 1) * width] = total.astype(jnp.bfloat16)
    sends.finish()


def mix(memory, conv, memory_weight, conv_weight):
    count, columns = lax.axis_size("sp"), lax.axis_size("tp")
    chunk, head_dim = memory.shape
    total, channels = conv.shape
    groups, share = count // ROLES, count // columns
    width = memory_weight.shape[1]
    length = total // count
    bf16 = jnp.bfloat16
    return pl.pallas_call(
        lambda *refs: mix_kernel(count, columns, *refs),
        out_shape=jax.ShapeDtypeStruct((length, width * share), bf16),
        in_specs=[IN_VMEM] * 4,
        out_specs=IN_VMEM,
        scratch_shapes=[
            pltpu.VMEM((groups, total, head_dim), bf16),
            pltpu.VMEM((groups, total, channels), bf16),
            pltpu.VMEM((total, width), bf16),
            pltpu.VMEM((share, columns, length, width), bf16),
            pltpu.SemaphoreType.DMA((96,)),
            pltpu.SemaphoreType.DMA((count,)),
            pltpu.SemaphoreType.DMA((count, ROLES)),
            pltpu.SemaphoreType.DMA((share, columns)),
        ],
        compiler_params=pltpu.CompilerParams(collective_id=2, has_side_effects=True),
    )(memory, conv, memory_weight, conv_weight)


def on_device_by_column(
    tokens,
    conv_value_weight,
    conv_gate_weight,
    conv_kernel,
    conv_norm_gain,
    query_weight,
    key_weight,
    value_weight,
    input_gate_weight,
    forget_gate_weight,
    input_offset,
    forget_offset,
    memory_norm_gain,
    conv_out_weight,
    memory_out_weight,
):
    f32, bf16 = jnp.float32, jnp.bfloat16
    count = lax.axis_size("sp")
    columns = lax.axis_size("tp")
    place = lax.axis_index("sp")
    heads_here = input_gate_weight.shape[1]
    head, role = place // ROLES, role_of(place)
    head_dim = query_weight.shape[1] // heads_here
    channels = conv_value_weight.shape[1] // heads_here
    gate_weights = jnp.concatenate([input_gate_weight, forget_gate_weight], axis=1)
    own_offsets = jnp.concatenate([input_offset, forget_offset], axis=1).T
    flat, gates, query, key, value, offsets = project(
        tokens,
        query_weight,
        key_weight,
        value_weight,
        conv_value_weight,
        conv_gate_weight,
        jnp.pad(gate_weights, ((0, 0), (0, 128 - 2 * heads_here))),
        jnp.pad(own_offsets, ((0, -2 * heads_here % 8), (0, 0))),
        head_dim,
    )
    length = flat.shape[0]
    offsets = offsets[:, : 2 * heads_here].transpose(1, 0, 2).reshape(2 * heads_here, length)
    gates = gates[:, : 2 * heads_here].T + offsets
    glu = (flat[:, :channels] * jax.nn.sigmoid(flat[:, channels:])).astype(bf16)
    taps = conv_kernel.shape[0]
    kernel = lax.dynamic_slice_in_dim(conv_kernel, head * channels, channels, 1).astype(f32)
    extended = jnp.concatenate([jnp.zeros((taps - 1, channels), f32), glu.astype(f32)], axis=0)
    conv = depthwise(extended, kernel)

    rows = length // ROLES
    start = role * rows
    gate_in = lax.dynamic_index_in_dim(gates[:heads_here], head, 0, False)
    forget_log = jax.nn.log_sigmoid(
        lax.dynamic_index_in_dim(gates[heads_here:], head, 0, False)
    )
    coarse, fine = forget_parts(forget_log)
    mine_coarse = lax.dynamic_slice_in_dim(coarse, start, rows)
    mine_fine = lax.dynamic_slice_in_dim(fine, start, rows)
    log_weight = (
        (mine_coarse[:, None] - coarse[None, :])
        + (mine_fine[:, None] - fine[None, :])
        + gate_in[None, :]
    )
    causal = (start + jnp.arange(rows))[:, None] >= jnp.arange(length)[None, :]
    log_weight = jnp.where(causal, log_weight, -jnp.inf)
    weight = jnp.exp(log_weight - jnp.max(log_weight, axis=1, keepdims=True))
    scores = jnp.einsum("td,sd->ts", query, key, preferred_element_type=f32) * (
        weight * head_dim ** (-0.5)
    )
    numer = jnp.dot(scores.astype(bf16), value, preferred_element_type=f32)
    denom = jnp.sum(scores, axis=1)
    cell = numer / jnp.maximum(jnp.abs(denom), 1.0)[:, None]

    squares = jnp.pad(jnp.sum(cell * cell, axis=1), (0, length - rows))
    normed = role == ROLES - 1
    sums = jnp.stack(
        [
            jnp.where(normed, jnp.sum(conv, axis=1), 0.0),
            jnp.where(normed, jnp.sum(conv * conv, axis=1), 0.0),
            squares,
        ]
    )
    sums = sum_over_group(jnp.pad(sums, ((0, 5), (0, 0))))
    total = conv_norm_gain.shape[0] * columns
    mean = sums[0] / total
    variance = sums[1] / total - mean * mean
    gain = lax.dynamic_slice_in_dim(conv_norm_gain, head * channels, channels)
    conv_branch = jax.nn.silu(
        (conv - mean[:, None]) * lax.rsqrt(variance + EPS)[:, None] * gain
    ).astype(bf16)
    entries = heads_here * head_dim * columns
    memory_scale = lax.rsqrt(sums[2, :rows] / entries + EPS)
    memory_gain = lax.dynamic_slice_in_dim(memory_norm_gain, head * head_dim, head_dim)
    memory_branch = (cell * memory_scale[:, None] * memory_gain).astype(bf16)

    return mix(memory_branch, conv_branch, memory_out_weight, conv_out_weight)


def splits_by_column(mesh, tokens, query_weight, conv_value_weight, input_gate_weight):
    count, columns = mesh.shape["sp"], mesh.shape["tp"]
    heads = input_gate_weight.shape[1]
    heads_here = heads // columns
    head_dim = query_weight.shape[1] // heads
    return (
        count == ROLES * heads_here
        and columns == 4
        and count % columns == 0
        and tokens.size * 2 <= 8 * 2**20
        and tokens.shape[0] % (count * 16) == 0
        and conv_value_weight.shape[1] * 2 == head_dim * heads
        and head_dim % 256 == 0
        and 2 * heads_here <= 128
    )


def solution(mesh):
    in_specs = (
        P("sp", "tp"),
        P("sp", "tp"),
        P("sp", "tp"),
        P(None, "tp"),
        P("tp"),
        P("sp", "tp"),
        P("sp", "tp"),
        P("sp", "tp"),
        P(None, "tp"),
        P(None, "tp"),
        P("sp", "tp"),
        P("sp", "tp"),
        P("tp"),
        P("tp", "sp"),
        P("tp", "sp"),
    )
    out_specs = P("sp", "tp")

    def run(*arrays):
        by_column = splits_by_column(mesh, arrays[0], arrays[5], arrays[1], arrays[8])
        on_device = on_device_by_column if by_column else on_device_by_position
        return jax.shard_map(
            on_device, mesh=mesh, in_specs=in_specs, out_specs=out_specs, check_vma=False
        )(*arrays)

    return run
```

```python
import jax
import jax.numpy as jnp
from jax import lax
from jax.experimental import pallas as pl
from jax.experimental.pallas import tpu as pltpu
from jax.sharding import PartitionSpec as P

BLOCK = 64


EPS = 1e-06
LOWEST_LEVEL = -1e30


def shifted_2(value, axis, steps):
    count = lax.axis_size(axis)
    leading, last = (max(0, -steps), min(count, count - steps))
    return lax.ppermute(value, axis, [(source, source + steps) for source in range(leading, last)])


def carried_in(shard, axis, join, neutral):
    place = lax.axis_index(axis)
    gathered = jax.tree.map(
        lambda a, kind: lax.all_gather(a.astype(kind), axis),
        shard,
        (jnp.bfloat16, jnp.bfloat16, jnp.bfloat16, jnp.bfloat16),
    )
    state = jax.tree.map(lambda a, e: jnp.zeros_like(a) + jnp.asarray(e, a.dtype), shard, neutral)

    def one(step, state):
        return join(
            state,
            jax.tree.map(
                lambda a, own: lax.dynamic_index_in_dim(a, step, 0, False).astype(own.dtype),
                gathered,
                shard,
            ),
        )

    return lax.fori_loop(0, place, one, state)


def block_step(carry, inputs):
    state, normal, level = carry
    query, key, value, gate_in, forget_log = inputs
    length = gate_in.shape[-1]
    scale = query.shape[-1] ** (-0.5)
    causal = jnp.tril(jnp.ones((length, length), dtype=bool))
    within = jnp.cumsum(forget_log, axis=-1)
    log_weight = within[:, :, None] - within[:, None, :] + gate_in[:, None, :]
    log_weight = jnp.where(causal, log_weight, -jnp.inf)
    carried = within + level[:, None]
    top = jnp.maximum(carried, jnp.max(log_weight, axis=-1))
    weight = jnp.exp(log_weight - top[:, :, None])
    carried_weight = jnp.exp(carried - top) * scale
    scores = jnp.einsum("htd,hsd->hts", query, key, preferred_element_type=jnp.float32) * (
        scale * weight
    )
    numer = jnp.einsum(
        "hts,hse->hte", scores.astype(jnp.bfloat16), value, preferred_element_type=jnp.float32
    )
    numer = numer + carried_weight[:, :, None] * jnp.einsum(
        "hed,htd->hte", state.astype(jnp.bfloat16), query, preferred_element_type=jnp.float32
    )
    denom = jnp.sum(scores, axis=-1) + carried_weight * jnp.einsum(
        "hd,htd->ht", normal.astype(jnp.bfloat16), query, preferred_element_type=jnp.float32
    )
    result = numer / jnp.maximum(jnp.abs(denom), 1.0)[:, :, None]
    last = within[:, -1]
    end_log = last[:, None] - within + gate_in
    new_level = jnp.maximum(last + level, jnp.max(end_log, axis=-1))
    keep = jnp.exp(last + level - new_level)
    fresh = jnp.exp(end_log - new_level[:, None])
    scaled_key = (fresh[:, :, None] * key).astype(jnp.bfloat16)
    new_state = keep[:, None, None] * state + jnp.einsum(
        "hse,hsd->hed", value, scaled_key, preferred_element_type=jnp.float32
    )
    new_normal = keep[:, None] * normal + jnp.sum(scaled_key.astype(jnp.float32), axis=1)
    return ((new_state, new_normal, new_level), result)


def depthwise(extended, kernel):
    taps = kernel.shape[0]
    length = extended.shape[0] - taps + 1
    total = extended[0:length] * kernel[0]
    for index in range(1, taps):
        total = total + extended[index : index + length] * kernel[index]
    return total


def merge_states(first, second):
    first_state, first_normal, first_level, first_total = first
    second_state, second_normal, second_level, second_total = second
    shifted = first_level + second_total
    level = jnp.maximum(shifted, second_level)
    older = jnp.exp(shifted - level)
    newer = jnp.exp(second_level - level)
    state = older[:, None, None] * first_state + newer[:, None, None] * second_state
    normal = older[:, None] * first_normal + newer[:, None] * second_normal
    return (state, normal, level, first_total + second_total)


def on_device_by_position(
    tokens,
    conv_value_weight,
    conv_gate_weight,
    conv_kernel,
    conv_norm_gain,
    query_weight,
    key_weight,
    value_weight,
    input_gate_weight,
    forget_gate_weight,
    input_offset,
    forget_offset,
    memory_norm_gain,
    conv_out_weight,
    memory_out_weight,
):
    length = tokens.shape[0]
    heads_here = input_gate_weight.shape[1]
    whole = lax.all_gather(tokens, "tp", axis=1, tiled=True)
    pieces = (
        lax.all_gather(conv_value_weight, "sp", axis=0, tiled=True),
        lax.all_gather(conv_gate_weight, "sp", axis=0, tiled=True),
        lax.all_gather(query_weight, "sp", axis=0, tiled=True),
        lax.all_gather(key_weight, "sp", axis=0, tiled=True),
        lax.all_gather(value_weight, "sp", axis=0, tiled=True),
    )
    folded = tuple((jnp.dot(whole, piece, preferred_element_type=jnp.float32) for piece in pieces))
    conv_value, conv_gate, query_flat, key_flat, value_flat = folded
    gate_pre = jnp.dot(whole, input_gate_weight, preferred_element_type=jnp.float32)
    forget_pre = jnp.dot(whole, forget_gate_weight, preferred_element_type=jnp.float32)
    glu = (conv_value * jax.nn.sigmoid(conv_gate)).astype(jnp.bfloat16)
    taps = conv_kernel.shape[0]
    head_dim = query_flat.shape[1] // heads_here

    def to_heads(flat):
        return flat.astype(jnp.bfloat16).reshape(length, heads_here, head_dim).transpose(1, 0, 2)

    query = to_heads(query_flat)
    key = to_heads(key_flat)
    value = to_heads(value_flat)
    gate_in = (gate_pre + input_offset).T
    forget_log = jax.nn.log_sigmoid(forget_pre + forget_offset).T
    within = jnp.cumsum(forget_log, axis=1)
    total = within[:, -1]
    end_log = total[:, None] - within + gate_in
    local_level = jnp.max(end_log, axis=1)
    fresh = jnp.exp(end_log - local_level[:, None])
    scaled_key = (fresh[:, :, None] * key).astype(jnp.bfloat16)
    local_state = jnp.einsum("hse,hsd->hed", value, scaled_key, preferred_element_type=jnp.float32)
    local_normal = jnp.sum(scaled_key.astype(jnp.float32), axis=1)
    blank_state = (
        jnp.zeros_like(local_state),
        jnp.zeros_like(local_normal),
        jnp.full_like(local_level, LOWEST_LEVEL),
        jnp.zeros_like(total),
    )
    prior = shifted_2(glu[length - (taps - 1) :], "sp", 1)
    incoming = carried_in(
        (local_state, local_normal, local_level, total), "sp", merge_states, blank_state
    )
    extended = jnp.concatenate([prior, glu], axis=0).astype(jnp.float32)
    conv = depthwise(extended, conv_kernel.astype(jnp.float32))
    blocks = length // BLOCK

    def split(array):
        return jnp.moveaxis(array.reshape((heads_here, blocks, BLOCK) + array.shape[2:]), 1, 0)

    _, hidden = lax.scan(
        block_step,
        tuple(incoming[:3]),
        (split(query), split(key), split(value), split(gate_in), split(forget_log)),
    )
    hidden = jnp.moveaxis(hidden, 0, 1).reshape(heads_here, length, head_dim)
    hidden_squares = jnp.sum(hidden * hidden, axis=(0, 2))
    channel_sum, channel_squares, memory_squares = lax.psum(
        (jnp.sum(conv, axis=1), jnp.sum(conv * conv, axis=1), hidden_squares), "tp"
    )
    channels = conv.shape[1] * lax.axis_size("tp")
    mean = (channel_sum / channels)[:, None]
    variance = (channel_squares / channels)[:, None] - mean * mean
    conv_branch = jax.nn.silu((conv - mean) * lax.rsqrt(variance + EPS) * conv_norm_gain).astype(
        jnp.bfloat16
    )
    entries = heads_here * head_dim * lax.axis_size("tp")
    memory_scale = lax.rsqrt(memory_squares / entries + EPS)
    hidden = hidden * memory_scale[None, :, None]
    hidden = hidden * memory_norm_gain.reshape(heads_here, 1, head_dim)
    memory_branch = (
        hidden.transpose(1, 0, 2).reshape(length, heads_here * head_dim).astype(jnp.bfloat16)
    )
    conv_columns, memory_columns = (
        lax.all_gather(conv_out_weight, "sp", axis=1, tiled=True),
        lax.all_gather(memory_out_weight, "sp", axis=1, tiled=True),
    )
    contract = (((0,), (1,)), ((), ()))
    summed = lax.psum_scatter(
        (
            lax.dot_general(conv_columns, conv_branch, contract, preferred_element_type=jnp.float32)
            + lax.dot_general(
                memory_columns, memory_branch, contract, preferred_element_type=jnp.float32
            )
        ).astype(jnp.bfloat16),
        "tp",
        scatter_dimension=0,
        tiled=True,
    ).astype(jnp.float32)
    return summed.T.astype(jnp.bfloat16)


def forget_parts(forget_log):
    coarse = jnp.round(forget_log * 8.0) * 0.125
    return jnp.cumsum(coarse, axis=-1), jnp.cumsum(forget_log - coarse, axis=-1)


MESH = pl.DeviceIdType.MESH
IN_VMEM = pl.BlockSpec(memory_space=pltpu.VMEM)
ROLES = 4


class Sends:
    def __init__(self, semaphores):
        self.semaphores = semaphores
        self.started = []

    def start(self, source, target, arrival, device, *conditions):
        semaphore = self.semaphores.at[len(self.started)]
        copy = pltpu.make_async_remote_copy(
            src_ref=source,
            dst_ref=target,
            send_sem=semaphore,
            recv_sem=arrival,
            device_id=device,
            device_id_type=MESH,
        )
        self.started.append((copy, conditions))
        when(conditions, copy.start)

    def finish(self):
        for copy, conditions in self.started:
            when(conditions, copy.wait_send)


def when(conditions, action):
    if not conditions:
        action()
        return
    every = conditions[0]
    for condition in conditions[1:]:
        every = jnp.logical_and(every, condition)
    pl.when(every)(action)


def arrived(block, semaphore, *conditions):
    copy = pltpu.make_async_remote_copy(
        src_ref=block,
        dst_ref=block,
        send_sem=semaphore,
        recv_sem=semaphore,
        device_id=(lax.axis_index("sp"), lax.axis_index("tp")),
        device_id_type=MESH,
    )
    when(conditions, copy.wait_recv)


def role_of(i):
    flip = lax.rem(i // ROLES, 2)
    return lax.rem(i, ROLES) + flip * (1 - 2 * lax.rem(i, 2))


def line_order(here, count):
    order = []
    for distance in range(1, count):
        order.append((here - distance, here >= distance, here + 1, here + 1 < count))
        order.append((here + distance, here + distance < count, here - 1, here > 0))
    return order


def project_kernel(
    count,
    columns,
    tokens,
    wq,
    wk,
    wv,
    wcv,
    wcg,
    gate_weights,
    own_offsets,
    flat,
    gates,
    query,
    key,
    value,
    offsets,
    whole,
    weights,
    mine,
    send_sem,
    token_sem,
    weight_sem,
    half_sem,
    group_sem,
    offset_sem,
):
    me, tp = lax.axis_index("sp"), lax.axis_index("tp")
    layers = count // 2
    z, x, y, core = me // 2, lax.rem(me, 2), tp // 2, lax.rem(tp, 2)
    length, features = tokens.shape
    depth = wq.shape[0]
    wide = weights.shape[1]
    narrow = wide // 2
    barrier = pltpu.get_barrier_semaphore()
    y_side, core_side = (1 - y) * 2 + core, y * 2 + 1 - core
    for step in range(1, count):
        pl.semaphore_signal(
            barrier, inc=1, device_id=(lax.rem(me + step, count), tp), device_id_type=MESH
        )
    for side in (y_side, core_side):
        pl.semaphore_signal(barrier, inc=1, device_id=(me, side), device_id_type=MESH)

    def block(i, j):
        return whole.at[
            pl.ds(pl.multiple_of(i * length, length), length),
            pl.ds(pl.multiple_of(j * features, features), features),
        ]

    whole[
        pl.ds(pl.multiple_of(me * length, length), length),
        pl.ds(pl.multiple_of(tp * features, features), features),
    ] = tokens[...]
    sends = Sends(send_sem)
    rows = pl.ds(pl.multiple_of(me * depth, depth), depth)
    pl.semaphore_wait(barrier, count + 1)

    def pass_on(i, j, source, sides, *conditions):
        for device in sides:
            sends.start(source, block(i, j), token_sem.at[i, j], device, *conditions)

    x_side = z * 2 + 1 - x
    sends.start(tokens, block(me, tp), token_sem.at[me, tp], (me - 2, tp), z > 0)
    sends.start(tokens, block(me, tp), token_sem.at[me, tp], (me + 2, tp), z + 1 < layers)
    pass_on(me, tp, tokens, ((x_side, tp), (me, y_side), (me, core_side)))
    for step in range(1, count):
        device = (lax.rem(me + step, count), tp)
        sends.start(own_offsets, offsets.at[me], offset_sem.at[me], device)
    offsets[me] = own_offsets[...]

    def send_weights():
        for step in range(1, count):
            target = lax.rem(me + step, count)
            head, role = target // ROLES, role_of(target)
            device = (target, tp)
            window = pl.ds(pl.multiple_of(head * wide, wide), wide)
            for index, source in enumerate((wq, wk, wv)):
                sends.start(
                    source.at[:, window],
                    weights.at[rows, :],
                    weight_sem.at[me],
                    device,
                    role == index,
                )
            window = pl.ds(pl.multiple_of(head * narrow, narrow), narrow)
            for side, (source, semaphore) in enumerate(((wcv, weight_sem), (wcg, half_sem))):
                place = weights.at[rows, side * narrow : (side + 1) * narrow]
                sends.start(source.at[:, window], place, semaphore.at[me], device, role == 3)

    for target in range(count):
        head, role = target // ROLES, (target % ROLES) ^ (target // ROLES % 2)

        @pl.when(me == target)
        def _():
            if role < 3:
                weights[rows, :] = (wq, wk, wv)[role][:, head * wide : (head + 1) * wide]
            else:
                weights[rows, :narrow] = wcv[:, head * narrow : (head + 1) * narrow]
                weights[rows, narrow:] = wcg[:, head * narrow : (head + 1) * narrow]

    order = line_order(z, layers)
    for index, (source, there, onward, further) in enumerate(order):
        if index == layers:
            send_weights()
        i = source * 2 + x
        arrived(block(i, tp), token_sem.at[i, tp], there)
        sends.start(
            block(i, tp), block(i, tp), token_sem.at[i, tp], (onward * 2 + x, tp), there, further
        )
        pass_on(i, tp, block(i, tp), ((x_side, tp), (me, y_side), (me, core_side)), there)
    for source, there in [(z, None)] + [entry[:2] for entry in order]:
        conditions = () if there is None else (there,)
        i = source * 2 + 1 - x
        arrived(block(i, tp), token_sem.at[i, tp], *conditions)
        pass_on(i, tp, block(i, tp), ((me, y_side), (me, core_side)), *conditions)
    for step in range(count):
        i = lax.rem(me + step, count)
        arrived(block(i, y_side), token_sem.at[i, y_side])
        pass_on(i, y_side, block(i, y_side), ((me, core_side),))
    for step in range(count):
        i = lax.rem(me + step, count)
        for j in (core_side, (1 - y) * 2 + 1 - core):
            arrived(block(i, j), token_sem.at[i, j])
    role_here = role_of(me)
    for step in range(1, count):
        i = lax.rem(me + step, count)
        arrived(offsets.at[i], offset_sem.at[i])
        part = pl.ds(pl.multiple_of(i * depth, depth), depth)
        arrived(weights.at[part, :], weight_sem.at[i], role_here < 3)
        arrived(weights.at[part, :narrow], weight_sem.at[i], role_here == 3)
        arrived(weights.at[part, narrow:], half_sem.at[i], role_here == 3)

    total = flat.shape[0]
    chunk = total // ROLES
    for index in range(ROLES):
        part = slice(index * chunk, (index + 1) * chunk)
        lines = whole[part, :]
        product = jnp.dot(lines, weights[...], preferred_element_type=jnp.float32)
        flat[part, :] = product
        mine[part, :] = product.astype(jnp.bfloat16)
        gates[part, :] = jnp.dot(lines, gate_weights[...], preferred_element_type=jnp.float32)

    first = me - lax.rem(me, ROLES)
    flip = lax.rem(me // ROLES, 2)
    for role in range(ROLES):
        part = slice(role * chunk, (role + 1) * chunk)
        until = slice(0, (role + 1) * chunk)
        device = (first + role + flip * (1 - 2 * (role % 2)), tp)
        for sender, target, source in (
            (2, value.at[until, :], mine.at[until, :]),
            (1, key.at[until, :], mine.at[until, :]),
            (0, query, mine.at[part, :]),
        ):
            if sender != role:
                sends.start(source, target, group_sem.at[sender], device, role_here == sender)
            else:

                @pl.when(role_here == role)
                def _():
                    target[...] = source[...]

        @pl.when(role_here == role)
        def _():
            if (role + 1) * chunk < total:
                rest = slice((role + 1) * chunk, total)
                key[rest, :] = jnp.zeros_like(key[rest, :])
                value[rest, :] = jnp.zeros_like(value[rest, :])

    for role in range(ROLES):
        until = slice(0, (role + 1) * chunk)
        for sender, target in ((0, query), (1, key.at[until, :]), (2, value.at[until, :])):
            if sender != role:
                arrived(target, group_sem.at[sender], role_here == role)
    sends.finish()


def project(tokens, wq, wk, wv, wcv, wcg, gate_weights, own_offsets, head_dim):
    count, columns = lax.axis_size("sp"), lax.axis_size("tp")
    length, features = tokens.shape
    total = length * count
    f32, bf16 = jnp.float32, jnp.bfloat16
    shape = jax.ShapeDtypeStruct
    return pl.pallas_call(
        lambda *refs: project_kernel(count, columns, *refs),
        out_shape=(
            shape((total, head_dim), f32),
            shape((total, gate_weights.shape[1]), f32),
            shape((total // ROLES, head_dim), bf16),
            shape((total, head_dim), bf16),
            shape((total, head_dim), bf16),
            shape((count,) + own_offsets.shape, f32),
        ),
        in_specs=[IN_VMEM] * 8,
        out_specs=(IN_VMEM,) * 6,
        scratch_shapes=[
            pltpu.VMEM((total, features * columns), bf16),
            pltpu.VMEM((wq.shape[0] * count, head_dim), bf16),
            pltpu.VMEM((total, head_dim), bf16),
            pltpu.SemaphoreType.DMA((192,)),
            pltpu.SemaphoreType.DMA((count, columns)),
            pltpu.SemaphoreType.DMA((count,)),
            pltpu.SemaphoreType.DMA((count,)),
            pltpu.SemaphoreType.DMA((3,)),
            pltpu.SemaphoreType.DMA((count,)),
        ],
        compiler_params=pltpu.CompilerParams(collective_id=0, has_side_effects=True),
    )(tokens, wq, wk, wv, wcv, wcg, gate_weights, own_offsets)


def sums_kernel(count, columns, sums, total, slots, send_sem, arrival_sem):
    me, tp = lax.axis_index("sp"), lax.axis_index("tp")
    groups = count // ROLES
    members = groups * columns
    role = role_of(me)
    own = (me // ROLES) * columns + tp
    barrier = pltpu.get_barrier_semaphore()
    peers = [lax.rem(own + step, members) for step in range(1, members)]
    devices = []
    for peer in peers:
        group = peer // columns
        seat = role + lax.rem(group, 2) * (1 - 2 * lax.rem(role, 2))
        devices.append((group * ROLES + seat, lax.rem(peer, columns)))
    for device in devices:
        pl.semaphore_signal(barrier, inc=1, device_id=device, device_id_type=MESH)
    pl.semaphore_wait(barrier, members - 1)
    sends = Sends(send_sem)
    for device in devices:
        sends.start(sums, slots.at[own], arrival_sem.at[own], device)
    slots[own] = sums[...]
    for peer in peers:
        arrived(slots.at[peer], arrival_sem.at[peer])
    result = slots[0]
    for index in range(1, members):
        result = result + slots[index]
    total[...] = result
    sends.finish()


def sum_over_group(sums):
    count, columns = lax.axis_size("sp"), lax.axis_size("tp")
    members = count // ROLES * columns
    return pl.pallas_call(
        lambda *refs: sums_kernel(count, columns, *refs),
        out_shape=jax.ShapeDtypeStruct(sums.shape, sums.dtype),
        in_specs=[IN_VMEM],
        out_specs=IN_VMEM,
        scratch_shapes=[
            pltpu.VMEM((members,) + sums.shape, sums.dtype),
            pltpu.SemaphoreType.DMA((members,)),
            pltpu.SemaphoreType.DMA((members,)),
        ],
        compiler_params=pltpu.CompilerParams(collective_id=1, has_side_effects=True),
    )(sums)


def mix_kernel(
    count,
    columns,
    memory,
    conv,
    memory_weight,
    conv_weight,
    mixed,
    memories,
    convs,
    partial,
    slots,
    send_sem,
    memory_sem,
    conv_sem,
    slot_sem,
):
    me, tp = lax.axis_index("sp"), lax.axis_index("tp")
    layers = count // 2
    z, x = me // 2, lax.rem(me, 2)
    chunk = memory.shape[0]
    share = count // columns
    barrier = pltpu.get_barrier_semaphore()
    for step in range(1, count):
        pl.semaphore_signal(
            barrier, inc=1, device_id=(lax.rem(me + step, count), tp), device_id_type=MESH
        )
    inside = me // share == tp
    for half in range(share):
        for j in range(columns):
            source = tp * share + half

            @pl.when(tp != j)
            def _():
                pl.semaphore_signal(barrier, inc=1, device_id=(source, j), device_id_type=MESH)

    @pl.when(inside)
    def _():
        pl.semaphore_wait(barrier, count - 1)

    @pl.when(jnp.logical_not(inside))
    def _():
        pl.semaphore_wait(barrier, 2 * count - 1)

    def memory_at(i):
        rows = pl.multiple_of(role_of(i) * chunk, chunk)
        return memories.at[i // ROLES, pl.ds(rows, chunk), :]

    def has_conv(i):
        return role_of(i) == ROLES - 1

    sends = Sends(send_sem)

    def piece(index):
        return slice(index * chunk, (index + 1) * chunk)

    def spread_memory(i, own, device, *conditions):
        sends.start(
            memory if own else memory_at(i), memory_at(i), memory_sem.at[i], device, *conditions
        )

    def spread_conv(i, index, own, device, *conditions):
        place = convs.at[i // ROLES, piece(index), :]
        sends.start(
            conv.at[piece(index), :] if own else place,
            place,
            conv_sem.at[i, index],
            device,
            has_conv(i),
            *conditions,
        )

    def conv_arrived(i, index, *conditions):
        place = convs.at[i // ROLES, piece(index), :]
        arrived(place, conv_sem.at[i, index], has_conv(i), *conditions)

    x_side = (z * 2 + 1 - x, tp)
    below, above = (me - 2, tp), (me + 2, tp)
    spread_memory(me, True, below, z > 0)
    spread_memory(me, True, above, z + 1 < layers)
    spread_memory(me, True, x_side)
    for index in range(ROLES):
        spread_conv(me, index, True, below, z > 0)
        spread_conv(me, index, True, above, z + 1 < layers)
        spread_conv(me, index, True, x_side)
    rows_here = pl.multiple_of(role_of(me) * chunk, chunk)
    memories[me // ROLES, pl.ds(rows_here, chunk), :] = memory[...]

    @pl.when(has_conv(me))
    def _():
        convs[me // ROLES] = conv[...]

    order = line_order(z, layers)
    for source, there, onward, further in order:
        i = source * 2 + x
        arrived(memory_at(i), memory_sem.at[i], there)
        spread_memory(i, False, (onward * 2 + x, tp), there, further)
        spread_memory(i, False, x_side, there)
    for source, there, onward, further in order:
        i = source * 2 + x
        for index in range(ROLES):
            conv_arrived(i, index, there)
            spread_conv(i, index, False, (onward * 2 + x, tp), there, further)
            spread_conv(i, index, False, x_side, there)
    for source, there in [(z, z >= 0)] + [entry[:2] for entry in order]:
        i = source * 2 + 1 - x
        arrived(memory_at(i), memory_sem.at[i], there)
        for index in range(ROLES):
            conv_arrived(i, index, there)

    groups = count // ROLES
    head_dim = memory.shape[1]
    channels = conv.shape[1]
    length = mixed.shape[0]
    for index in range(ROLES):
        part = slice(index * chunk, (index + 1) * chunk)
        total = None
        for head in range(groups):
            term = jnp.dot(
                memories[head, part, :],
                memory_weight[head * head_dim : (head + 1) * head_dim, :],
                preferred_element_type=jnp.float32,
            ) + jnp.dot(
                convs[head, part, :],
                conv_weight[head * channels : (head + 1) * channels, :],
                preferred_element_type=jnp.float32,
            )
            total = term if total is None else total + term
        partial[part, :] = total.astype(jnp.bfloat16)
    column, half = me // share, lax.rem(me, share)
    for step in range(count):
        i = lax.rem(me + step, count)
        place = pl.ds(pl.multiple_of(i * length, length), length)
        away = jnp.logical_or(i != me, tp != column)
        sends.start(
            partial.at[place, :], slots.at[half, tp], slot_sem.at[half, tp], (i, column), away
        )
        if step == 0:

            @pl.when(jnp.logical_not(away))
            def _():
                slots[half, tp] = partial[place, :]

    width = partial.shape[1]
    for half in range(share):
        total = None
        for j in range(columns):
            arrived(
                slots.at[half, j],
                slot_sem.at[half, j],
                jnp.logical_or(tp * share + half != me, tp != j),
            )
        for j in range(columns):
            term = slots[half, j].astype(jnp.float32)
            total = term if total is None else total + term
        mixed[:, half * width : (half + 1) * width] = total.astype(jnp.bfloat16)
    sends.finish()


def mix(memory, conv, memory_weight, conv_weight):
    count, columns = lax.axis_size("sp"), lax.axis_size("tp")
    chunk, head_dim = memory.shape
    total, channels = conv.shape
    groups, share = count // ROLES, count // columns
    width = memory_weight.shape[1]
    length = total // count
    bf16 = jnp.bfloat16
    return pl.pallas_call(
        lambda *refs: mix_kernel(count, columns, *refs),
        out_shape=jax.ShapeDtypeStruct((length, width * share), bf16),
        in_specs=[IN_VMEM] * 4,
        out_specs=IN_VMEM,
        scratch_shapes=[
            pltpu.VMEM((groups, total, head_dim), bf16),
            pltpu.VMEM((groups, total, channels), bf16),
            pltpu.VMEM((total, width), bf16),
            pltpu.VMEM((share, columns, length, width), bf16),
            pltpu.SemaphoreType.DMA((96,)),
            pltpu.SemaphoreType.DMA((count,)),
            pltpu.SemaphoreType.DMA((count, ROLES)),
            pltpu.SemaphoreType.DMA((share, columns)),
        ],
        compiler_params=pltpu.CompilerParams(collective_id=2, has_side_effects=True),
    )(memory, conv, memory_weight, conv_weight)


def on_device_by_column(
    tokens,
    conv_value_weight,
    conv_gate_weight,
    conv_kernel,
    conv_norm_gain,
    query_weight,
    key_weight,
    value_weight,
    input_gate_weight,
    forget_gate_weight,
    input_offset,
    forget_offset,
    memory_norm_gain,
    conv_out_weight,
    memory_out_weight,
):
    f32, bf16 = jnp.float32, jnp.bfloat16
    count = lax.axis_size("sp")
    columns = lax.axis_size("tp")
    place = lax.axis_index("sp")
    heads_here = input_gate_weight.shape[1]
    head, role = place // ROLES, role_of(place)
    head_dim = query_weight.shape[1] // heads_here
    channels = conv_value_weight.shape[1] // heads_here
    gate_weights = jnp.concatenate([input_gate_weight, forget_gate_weight], axis=1)
    own_offsets = jnp.concatenate([input_offset, forget_offset], axis=1).T
    flat, gates, query, key, value, offsets = project(
        tokens,
        query_weight,
        key_weight,
        value_weight,
        conv_value_weight,
        conv_gate_weight,
        jnp.pad(gate_weights, ((0, 0), (0, 128 - 2 * heads_here))),
        jnp.pad(own_offsets, ((0, -2 * heads_here % 8), (0, 0))),
        head_dim,
    )
    length = flat.shape[0]
    offsets = offsets[:, : 2 * heads_here].transpose(1, 0, 2).reshape(2 * heads_here, length)
    gates = gates[:, : 2 * heads_here].T + offsets
    glu = (flat[:, :channels] * jax.nn.sigmoid(flat[:, channels:])).astype(bf16)
    taps = conv_kernel.shape[0]
    kernel = lax.dynamic_slice_in_dim(conv_kernel, head * channels, channels, 1).astype(f32)
    extended = jnp.concatenate([jnp.zeros((taps - 1, channels), f32), glu.astype(f32)], axis=0)
    conv = depthwise(extended, kernel)

    rows = length // ROLES
    start = role * rows
    gate_in = lax.dynamic_index_in_dim(gates[:heads_here], head, 0, False)
    forget_log = jax.nn.log_sigmoid(
        lax.dynamic_index_in_dim(gates[heads_here:], head, 0, False)
    )
    coarse, fine = forget_parts(forget_log)
    mine_coarse = lax.dynamic_slice_in_dim(coarse, start, rows)
    mine_fine = lax.dynamic_slice_in_dim(fine, start, rows)
    log_weight = (
        (mine_coarse[:, None] - coarse[None, :])
        + (mine_fine[:, None] - fine[None, :])
        + gate_in[None, :]
    )
    causal = (start + jnp.arange(rows))[:, None] >= jnp.arange(length)[None, :]
    log_weight = jnp.where(causal, log_weight, -jnp.inf)
    weight = jnp.exp(log_weight - jnp.max(log_weight, axis=1, keepdims=True))
    scores = jnp.einsum("td,sd->ts", query, key, preferred_element_type=f32) * (
        weight * head_dim ** (-0.5)
    )
    numer = jnp.dot(scores.astype(bf16), value, preferred_element_type=f32)
    denom = jnp.sum(scores, axis=1)
    cell = numer / jnp.maximum(jnp.abs(denom), 1.0)[:, None]

    squares = jnp.pad(jnp.sum(cell * cell, axis=1), (0, length - rows))
    normed = role == ROLES - 1
    sums = jnp.stack(
        [
            jnp.where(normed, jnp.sum(conv, axis=1), 0.0),
            jnp.where(normed, jnp.sum(conv * conv, axis=1), 0.0),
            squares,
        ]
    )
    sums = sum_over_group(jnp.pad(sums, ((0, 5), (0, 0))))
    total = conv_norm_gain.shape[0] * columns
    mean = sums[0] / total
    variance = sums[1] / total - mean * mean
    gain = lax.dynamic_slice_in_dim(conv_norm_gain, head * channels, channels)
    conv_branch = jax.nn.silu(
        (conv - mean[:, None]) * lax.rsqrt(variance + EPS)[:, None] * gain
    ).astype(bf16)
    entries = heads_here * head_dim * columns
    memory_scale = lax.rsqrt(sums[2, :rows] / entries + EPS)
    memory_gain = lax.dynamic_slice_in_dim(memory_norm_gain, head * head_dim, head_dim)
    memory_branch = (cell * memory_scale[:, None] * memory_gain).astype(bf16)

    return mix(memory_branch, conv_branch, memory_out_weight, conv_out_weight)


def splits_by_column(mesh, tokens, query_weight, conv_value_weight, input_gate_weight):
    count, columns = mesh.shape["sp"], mesh.shape["tp"]
    heads = input_gate_weight.shape[1]
    heads_here = heads // columns
    head_dim = query_weight.shape[1] // heads
    return (
        count == ROLES * heads_here
        and columns == 4
        and count % columns == 0
        and tokens.size * 2 <= 8 * 2**20
        and tokens.shape[0] % (count * 16) == 0
        and conv_value_weight.shape[1] * 2 == head_dim * heads
        and head_dim % 256 == 0
        and 2 * heads_here <= 128
    )


def solution(mesh):
    in_specs = (
        P("sp", "tp"),
        P("sp", "tp"),
        P("sp", "tp"),
        P(None, "tp"),
        P("tp"),
        P("sp", "tp"),
        P("sp", "tp"),
        P("sp", "tp"),
        P(None, "tp"),
        P(None, "tp"),
        P("sp", "tp"),
        P("sp", "tp"),
        P("tp"),
        P("tp", "sp"),
        P("tp", "sp"),
    )
    out_specs = P("sp", "tp")

    def run(*arrays):
        by_column = splits_by_column(mesh, arrays[0], arrays[5], arrays[1], arrays[8])
        on_device = on_device_by_column if by_column else on_device_by_position
        return jax.shard_map(
            on_device, mesh=mesh, in_specs=in_specs, out_specs=out_specs, check_vma=False
        )(*arrays)

    return run
```
